1024 devices in a mesh: ep: 64 (over z, y), tp: 16 (over x, core).
Axes of the slice: x: 8, y: 8, z: 8, core: 2. Of those that a mesh axis runs over, the one named last changes fastest.
Arguments:
- tokens: bfloat16 [8192, 2048], P('ep'), may hold values from -6 to 6
- out_grad: bfloat16 [8192, 2048], P('ep'), may hold values from -50 to 50
- expert_ids: int32 [8192, 2], P('ep'), may hold values from 0 to 63, all different within a row; in each aligned block of 128 rows (0 to 127, 128 to 255, ...) at most 5 rows name the same one
- route_weights: float32 [8192, 2], P('ep'), may hold values from 0.2 to 2
- gate_proj: bfloat16 [64, 2048, 2048], P('ep', 'tp'), may hold values from -0.125 to 0.125
- up_proj: bfloat16 [64, 2048, 2048], P('ep', 'tp'), may hold values from -0.125 to 0.125
- down_proj: bfloat16 [64, 2048, 2048], P('ep', 'tp'), may hold values from -0.125 to 0.125
- shared_act: bfloat16 [8192, 1024], P('ep'), may hold values from -0.29882812 to 0.29882812
Outputs:
- token_grad: bfloat16 [8192, 2048], P('ep', 'tp')
- route_grad: float32 [8192, 2], P('ep')
- gate_grad: bfloat16 [64, 2048, 2048], P('ep', 'tp')
- up_grad: bfloat16 [64, 2048, 2048], P('ep', 'tp')
- down_grad: bfloat16 [64, 2048, 2048], P('ep', 'tp')
- row_norms: float32 [64, 3, 2048], P('ep', None, 'tp')
- shared_grad: float32 [1024, 2048], P('tp', 'ep')
- shared_norms: float32 [1024], P('tp')
The draws below stay inside these ranges and needn't reach their ends.
Inputs may be any that keep to these rules, and one draw needn't show every extreme that they name: `expert_ids`: each row names 2 different experts. In the rows of one device no expert is named more than 5 times, and in some device some expert is named exactly 5 times.
All inputs are finite; a program needn't handle non-finite values.
Results may differ from the reference program's by a relative error of at most 0.008.
Values may be sent and summed in bfloat16 or wider, within the bound.
No kernel may reach another device: no remote copies, remote signals or barrier semaphores. Data moves between devices by JAX's collectives and lax.ppermute only.
A program may use at most 32 MiB of HBM per device.

```python
import math
import jax
import jax.numpy as jnp
import numpy as np
from jax import lax

D = 2048
F = 2048
SH = 1024
TOPK = 2
TOK_DEV = 128
EXPERTS = 64
TOKENS = 8192
CAP = 5
N_EP = 64
N_TP = 16


def draw_out_grad(key, part):
    key_cols = jax.random.fold_in(key, 11)
    key_rows = jax.random.fold_in(key, 12)
    key_base = jax.random.fold_in(key, 13)
    position = jnp.arange(D, dtype=jnp.float32) / max(D - 1, 1)
    col_scale = jnp.exp(position * jnp.log(3.0)) * jnp.exp(jax.random.uniform(key_cols, (D,), jnp.float32, -1.2, 1.2))
    row_scale = jnp.exp(jax.random.uniform(key_rows, (TOKENS, 1), jnp.float32, -1.2, 1.2))
    base = jnp.clip(jax.random.normal(key_base, (TOKENS, D), jnp.float32), -6.0, 6.0)
    return (0.25 * base * row_scale * col_scale[None, :]).astype(jnp.bfloat16)


def steps_of(own_key, extent, shards, smallest, top_value):
    loudness, own = 1.0, jax.random.fold_in(own_key, 6)
    for axis_at, shards_of in shards:
        steps = jnp.exp(jax.random.uniform(jax.random.fold_in(own, axis_at), (shards_of,), jnp.float32, smallest / len(shards), top_value / len(shards)))
        loudness = loudness * jnp.repeat(steps, extent[axis_at] // shards_of).reshape([-1 if axis == axis_at else 1 for axis in range(len(extent))])
    return loudness


def routed_block(key, own, number, rows, amount, top, most, lean):
    ranking = jax.random.permutation(key, amount)
    crowded, usual = load_shares(amount, rows * top, most, lean, True), load_shares(amount, rows * top, most, lean, False)
    places = jnp.arange(amount)

    def named(tallies, offset_by):
        used = int((tallies > 0).sum())
        fixed = max(1, used // 4)
        moved = fixed + (places - fixed + offset_by * (used - fixed)) % max(1, amount - fixed)
        return jnp.zeros((amount,), jnp.int32).at[ranking[jnp.where(places < fixed, places, moved)]].set(jnp.asarray(tallies, jnp.int32))

    tallies = jnp.where(number % 4 == 0, named(crowded, number // 4), named(usual, number - number // 4 - 1))
    mixed = jax.random.permutation(jax.random.fold_in(own, 3), amount)
    donor, taker = mixed[0:amount // 2 * 2:2], mixed[1:amount // 2 * 2:2]
    slack = jnp.minimum(tallies[donor] - 1, most - tallies[taker]) // 2
    slack = jnp.where((donor == ranking[0]) | (taker == ranking[0]) | (tallies[taker] == 0), 0, jnp.maximum(slack, 0))
    moved = jax.random.randint(jax.random.fold_in(own, 4), (amount // 2,), 0, 1 << 20) % (slack + 1)
    tallies = tallies.at[donor].add(-moved).at[taker].add(moved)
    members = jnp.searchsorted(jnp.cumsum(tallies), jnp.arange(rows * top), side="right").astype(jnp.int32)
    listing = members.reshape(top, rows).T
    listing = listing[jax.random.permutation(jax.random.fold_in(own, 1), rows)]
    offset_by = jax.random.randint(jax.random.fold_in(own, 2), (rows, 1), 0, top)
    return jnp.take_along_axis(listing, (jnp.arange(top)[None, :] + offset_by) % top, axis=1)


def load_shares(count, total, bound, lean, full):
    portions = [(1 << 20) // math.isqrt(rank ** lean) + 1 for rank in range(1, count + 1)]
    largest = bound if full else min(bound, max(-(-total // count), total * portions[0] // sum(portions)))
    least = 1 if total - largest >= count - 1 else 0
    counts, spare = [largest] + [least] * (count - 1), total - largest - least * (count - 1)
    while spare > 0:
        candidates = [i for i in range(1, count) if counts[i] < largest] or [i for i in range(1, count) if counts[i] < bound]
        pool, budget = sum([portions[i] for i in candidates]), spare
        for i in candidates:
            more = min(bound - counts[i], max(1, budget * portions[i] // pool), spare)
            counts[i] = counts[i] + more
            spare = spare - more
    return np.array(counts)


def scatter_about(rng, dims, scale, bound, split=(), kind=jnp.bfloat16):
    entries = jax.random.normal(rng, dims, jnp.float32) * scale
    if len(split) > 0:
        entries = steps_of(rng, dims, split, -0.22, 0.18) * entries
    return jnp.clip(entries, min=-bound, max=bound).astype(kind)


def setup_inputs(seed: int = 0) -> dict:
    keys = jax.random.split(jax.random.key(seed), 9)
    tokens = scatter_about(keys[0], (TOKENS, D), 1.0, 6.0, ((0, 64),))
    out_grad = draw_out_grad(jax.random.fold_in(keys[8], 71), 0)
    expert_ids_keys = jax.random.split(jax.random.fold_in(keys[2], 1), TOKENS // TOK_DEV)
    expert_ids_turns = jax.random.permutation(jax.random.fold_in(keys[2], 3), TOKENS // TOK_DEV)
    expert_ids = jax.vmap(lambda own, number: routed_block(jax.random.fold_in(keys[2], 2), own, number, TOK_DEV, EXPERTS, TOPK, CAP, 2))(expert_ids_keys, expert_ids_turns).reshape((TOKENS, TOPK))
    route_weights = jnp.clip(jnp.exp(math.log(2.0) - 2.3025851 * jax.random.uniform(keys[3], (TOKENS, TOPK), jnp.float32) ** steps_of(keys[3], (TOKENS, TOPK), ((0, 64),), -0.2, 0.2)), 0.2, 2.0)
    gate_proj = scatter_about(keys[4], (EXPERTS, F, D), D ** -0.5, 0.125, ((0, 64), (1, 16)))
    up_proj = scatter_about(keys[5], (EXPERTS, F, D), D ** -0.5, 0.125, ((0, 64), (1, 16)))
    down_proj = scatter_about(keys[6], (EXPERTS, F, D), D ** -0.5, 0.125, ((0, 64), (1, 16)))
    shared_act = scatter_about(keys[7], (TOKENS, SH), 0.05, 0.29882812, ((0, 64),))
    return {"tokens": tokens, "out_grad": out_grad, "expert_ids": expert_ids, "route_weights": route_weights, "gate_proj": gate_proj, "up_proj": up_proj, "down_proj": down_proj, "shared_act": shared_act}


def expert_pass(tokens, scaled, index_row, gate_w, up_w, down_w):
    valid = index_row >= 0
    safe = jnp.where(valid, index_row, 0)
    rows_in = jnp.where(valid[:, None], tokens[safe // TOPK], jnp.zeros((), tokens.dtype))
    rows_cot = jnp.where(valid[:, None], scaled[safe], jnp.zeros((), scaled.dtype))
    gate_pre = jnp.dot(rows_in, gate_w.T, preferred_element_type=jnp.float32)
    up_pre = jnp.dot(rows_in, up_w.T, preferred_element_type=jnp.float32)
    sigmoid_a = jax.nn.sigmoid(gate_pre)
    silu_a = gate_pre * sigmoid_a
    hidden = (silu_a * up_pre).astype(jnp.bfloat16)
    hidden_grad = jnp.dot(rows_cot, down_w.T, preferred_element_type=jnp.float32)
    up_delta = (hidden_grad * silu_a).astype(jnp.bfloat16)
    gate_delta = (hidden_grad * up_pre * sigmoid_a * (1.0 + gate_pre * (1.0 - sigmoid_a))).astype(jnp.bfloat16)
    gate_full = jnp.dot(gate_delta.T, rows_in, preferred_element_type=jnp.float32)
    up_full = jnp.dot(up_delta.T, rows_in, preferred_element_type=jnp.float32)
    down_full = jnp.dot(hidden.T, rows_cot, preferred_element_type=jnp.float32)
    norm_rows = jnp.stack([jnp.sum(gate_full * gate_full, 1), jnp.sum(up_full * up_full, 1),
                           jnp.sum(down_full * down_full, 1)])
    row_count = index_row.shape[0]
    block = F // N_TP
    partial_value = jnp.einsum('rbf,bfd->rbd', gate_delta.astype(jnp.float32).reshape(row_count, N_TP, block),
                         gate_w.astype(jnp.float32).reshape(N_TP, block, D))
    partial_value = partial_value + jnp.einsum('rbf,bfd->rbd', up_delta.astype(jnp.float32).reshape(row_count, N_TP, block),
                                   up_w.astype(jnp.float32).reshape(N_TP, block, D))
    partial_value = lax.optimization_barrier(partial_value.astype(jnp.bfloat16)).astype(jnp.float32)
    slot_grad = jnp.sum(partial_value, 1)
    inner_part = (hidden.astype(jnp.float32) * hidden_grad).reshape(row_count, N_TP, block).sum(-1)
    inner_part = lax.optimization_barrier(inner_part.astype(jnp.bfloat16)).astype(jnp.float32)
    inner = jnp.sum(inner_part, 1)
    return (gate_full.astype(jnp.bfloat16), up_full.astype(jnp.bfloat16), down_full.astype(jnp.bfloat16),
            norm_rows, slot_grad, inner)


def reference(tokens, out_grad, expert_ids, route_weights, gate_proj, up_proj, down_proj, shared_act):
    per_dev = TOK_DEV * TOPK
    chosen = expert_ids.reshape(N_EP, per_dev).astype(jnp.int32)
    onehot = (chosen[..., None] == jnp.arange(EXPERTS, dtype=jnp.int32)[None, None, :]).astype(jnp.int32)
    before = jnp.cumsum(onehot, axis=1) - onehot
    rank_in = jnp.sum(before * onehot, -1).astype(jnp.int32)
    row_at = (jnp.arange(N_EP, dtype=jnp.int32)[:, None] * CAP + rank_in).astype(jnp.int32)
    global_id = jnp.arange(N_EP * per_dev, dtype=jnp.int32).reshape(N_EP, per_dev)
    table = jnp.full((EXPERTS, N_EP * CAP), -1, jnp.int32).at[chosen, row_at].set(global_id)
    scaled = (route_weights[:, :, None] * out_grad[:, None, :].astype(jnp.float32)).astype(jnp.bfloat16)
    scaled = scaled.reshape(TOKENS * TOPK, D)

    def one_expert(packed):
        index_row, gate_w, up_w, down_w = packed
        return expert_pass(tokens, scaled, index_row, gate_w, up_w, down_w)

    gate_grad, up_grad, down_grad, row_norms, slot_grads, inners = lax.map(
        one_expert, (table, gate_proj, up_proj, down_proj))
    target = jnp.where(table >= 0, table, TOKENS * TOPK).reshape(-1)
    assign_grad = jnp.zeros((TOKENS * TOPK + 1, D), jnp.float32).at[target].add(slot_grads.reshape(-1, D))
    assign_inner = jnp.zeros((TOKENS * TOPK + 1,), jnp.float32).at[target].add(inners.reshape(-1))
    token_grad = assign_grad[:TOKENS * TOPK].reshape(TOKENS, TOPK, D).sum(1).astype(jnp.bfloat16)
    route_grad = assign_inner[:TOKENS * TOPK].reshape(TOKENS, TOPK) / route_weights
    shared_grad = jnp.dot(shared_act.T, out_grad, preferred_element_type=jnp.float32)
    shared_norms = jnp.sum(shared_grad * shared_grad, 1)
    return (token_grad, route_grad, gate_grad, up_grad, down_grad, row_norms, shared_grad, shared_norms)
```

```python
import functools

import jax
import jax.numpy as jnp
from jax import lax
from jax.experimental import pallas as pl
from jax.experimental.pallas import tpu as pltpu
from jax.sharding import Mesh
from jax.sharding import PartitionSpec as P

EP = ("z", "y")
TP = ("x", "c")
BF, F32, I32 = jnp.bfloat16, jnp.float32, jnp.int32
LANES = 128
TILE = 8
HALF = TILE * LANES
SHARED = 2


def params(mib):
    return pltpu.CompilerParams(vmem_limit_bytes=mib * 1024 * 1024)


def in_vmem(n):
    return [pl.BlockSpec(memory_space=pltpu.VMEM)] * n


def in_smem(n):
    return [pl.BlockSpec(memory_space=pltpu.SMEM)] * n


def iota(shape, dim):
    return lax.broadcasted_iota(I32, shape, dim)


def ones_at(mask):
    return mask.astype(F32).astype(BF)


def dot(a, b, ca=1, cb=0):
    return lax.dot_general(a, b, (((ca,), (cb,)), ((), ())), preferred_element_type=F32)


def split2(v):
    hi = v.astype(BF).astype(F32)
    return hi, v - hi


def spread(ref, x):
    for j in range(TILE):
        cols = x[:, j * LANES : (j + 1) * LANES].astype(F32)
        ref[pl.ds(j, x.shape[0], stride=TILE), :] = cols


def gather_cols(ref, count, j):
    return ref[pl.ds(j, count, stride=TILE), :]


def send_kernel(
    cap, ids_s, w_s, at_s, tok_ref, grad_ref, act_ref, out_ref, rank_s, seen_s, tok_t, grad_t
):
    count, width = grad_ref.shape
    experts = out_ref.shape[0]
    mine = pl.ds(pl.multiple_of((at_s[0] % 2) * HALF, HALF), HALF)
    spread(tok_t, tok_ref[:, mine])
    spread(grad_t, grad_ref[:, mine])
    for e in range(experts):
        seen_s[e] = 0
    out_ref[:, : 2 * cap] = jnp.zeros((experts, 2 * cap, TILE, LANES), BF)

    def one_token(t, carry):
        rows = pl.ds(pl.multiple_of(t * TILE, TILE), TILE)
        tok = tok_t[rows, :].astype(BF)
        grad = grad_t[rows, :]
        for k in range(2):
            e = ids_s[k, t]
            r = seen_s[e]
            seen_s[e] = r + 1
            rank_s[k, t] = r
            out_ref[e, r] = tok
            out_ref[e, cap + r] = (w_s[k, t] * grad).astype(BF)
        return carry

    lax.fori_loop(0, count, one_token, 0, unroll=8)

    half = LANES // 2
    act = act_ref[:, pl.ds(pl.multiple_of((at_s[0] // 2) * LANES, LANES), LANES)]
    swapped = jnp.concatenate([act[:, half:], act[:, :half]], axis=1)
    left = iota(act.shape, 1) < half
    own = (at_s[0] % 2) * half
    keep = (iota(act.shape, 1) // half) * half == own
    twice = jnp.where(keep, act.astype(F32), swapped.astype(F32)).astype(BF)
    step = 2 * LANES
    block = width // experts
    for s in range(0, width, step):
        term = dot(grad_ref[:, s : s + step], twice, 0, 0)
        term = term.reshape(step // block, 2, block // 2, LANES)
        lane = iota((step // block, block // 2, LANES), 2)
        both = jnp.where(lane < half, term[:, 0], term[:, 1]).astype(BF)
        out_ref[s // block : (s + step) // block, 2 * cap :] = both.reshape(
            step // block, SHARED, TILE, LANES
        )


def send_rows(ids_t, w_t, at, tokens, out_grad, act, cap, experts):
    count = tokens.shape[0]
    return pl.pallas_call(
        functools.partial(send_kernel, cap),
        in_specs=in_smem(3) + in_vmem(3),
        out_specs=in_vmem(1) + in_smem(1),
        out_shape=[
            jax.ShapeDtypeStruct((experts, 2 * cap + SHARED, TILE, LANES), BF),
            jax.ShapeDtypeStruct((2, count), I32),
        ],
        scratch_shapes=[
            pltpu.SMEM((experts,), I32),
            pltpu.VMEM((count * TILE, LANES), F32),
            pltpu.VMEM((count * TILE, LANES), F32),
        ],
        compiler_params=params(16),
        name="send_rows",
    )(ids_t, w_t, at, tokens, out_grad, act)


def unpack_kernel(cap, recv_ref, rows_ref, in_t, cot_t):
    n = recv_ref.shape[0]
    count = n * cap
    for k, ref in enumerate((in_t, cot_t)):
        tiles = recv_ref[:, k * cap : (k + 1) * cap].astype(F32)
        ref[...] = tiles.reshape(count * TILE, LANES)
        for j in range(TILE):
            cols = slice(j * LANES, (j + 1) * LANES)
            rows_ref[k, :, cols] = gather_cols(ref, count, j).astype(BF)


def unpack(recv, cap):
    count = recv.shape[0] * cap
    return pl.pallas_call(
        functools.partial(unpack_kernel, cap),
        in_specs=in_vmem(1),
        out_specs=pl.BlockSpec(memory_space=pltpu.VMEM),
        out_shape=jax.ShapeDtypeStruct((2, count, HALF), BF),
        scratch_shapes=[pltpu.VMEM((count * TILE, LANES), F32)] * 2,
        compiler_params=params(16),
        name="unpack",
    )(recv)


def shared_kernel(cap, recv_ref, out_ref, norm_ref):
    n = recv_ref.shape[0]
    total = jnp.sum(recv_ref[:, 2 * cap :].astype(F32), axis=0).reshape(SHARED * TILE, LANES)
    half = LANES // 2
    out_ref[...] = jnp.concatenate([total[:, :half], total[:, half:]], axis=0)
    sq = jnp.sum(total * total, axis=0, keepdims=True)
    sq = sq + jnp.concatenate([sq[:, half:], sq[:, :half]], axis=1)
    norm_ref[...] = jnp.broadcast_to(sq, norm_ref.shape)


def shared_sum(recv, cap):
    return pl.pallas_call(
        functools.partial(shared_kernel, cap),
        in_specs=in_vmem(1),
        out_specs=in_vmem(2),
        out_shape=[
            jax.ShapeDtypeStruct((2 * SHARED * TILE, LANES // 2), F32),
            jax.ShapeDtypeStruct((TILE, LANES), F32),
        ],
        compiler_params=params(16),
        name="shared_sum",
    )(recv)


def forward_kernel(core_s, own_ref, other_ref, gate_ref, up_ref, down_ref, keep_ref, give_ref, delta_ref):
    core = core_s[0]
    count = own_ref.shape[1]
    gate_pre = up_pre = hidden_grad = 0.0
    step = 2 * LANES
    for side, ref in ((core, own_ref), (1 - core, other_ref)):
        for s in range(0, HALF, step):
            cols = pl.ds(pl.multiple_of(side * HALF + s, step), step)
            a, b = ref[0, :, s : s + step], ref[1, :, s : s + step]
            gate_pre = gate_pre + dot(a, gate_ref[0, :, cols], 1, 1)
            up_pre = up_pre + dot(a, up_ref[0, :, cols], 1, 1)
            hidden_grad = hidden_grad + dot(b, down_ref[0, :, cols], 1, 1)
    sig = jax.nn.sigmoid(gate_pre)
    silu = gate_pre * sig
    hidden = (silu * up_pre).astype(BF)
    up_delta = (hidden_grad * silu).astype(BF)
    gate_delta = (hidden_grad * up_pre * sig * (1.0 + gate_pre * (1.0 - sig))).astype(BF)
    both = jnp.concatenate([gate_delta, up_delta], axis=1)
    for ref, side in ((give_ref, 1 - core), (keep_ref, core)):
        for j in range(TILE):
            cols = pl.ds(pl.multiple_of(j * step + side * LANES, LANES), LANES)
            w = jnp.concatenate([gate_ref[0, :, cols], up_ref[0, :, cols]], axis=0)
            ref[:count, j * LANES : (j + 1) * LANES] = dot(both, w).astype(BF)
    for k, d in enumerate((gate_delta, up_delta, hidden)):
        delta_ref[k] = d.astype(F32).T.astype(BF)
    inner = jnp.sum(hidden.astype(F32) * hidden_grad, axis=1, keepdims=True)
    spot = iota((count, LANES), 0) % LANES == iota((count, LANES), 1)
    spots = jnp.where(spot, inner, 0.0)
    lines = [
        jnp.sum(spots[s : min(s + LANES, count)], axis=0, keepdims=True)
        for s in range(0, count, LANES)
    ]
    hi, lo = split2(jnp.concatenate(lines, axis=0))
    pad = jnp.zeros((TILE - 2 * len(lines), LANES), F32)
    tile = jnp.concatenate([hi, lo, pad], axis=0).astype(BF)
    for ref in (keep_ref, give_ref):
        ref[count:, :] = jnp.zeros((TILE, HALF), BF)
        ref[count:, :LANES] = tile


def forward(core, own, other, gate, up, down):
    count = own.shape[1]
    part = jax.ShapeDtypeStruct((count + TILE, HALF), BF)
    return pl.pallas_call(
        forward_kernel,
        in_specs=in_smem(1) + in_vmem(5),
        out_specs=in_vmem(3),
        out_shape=[part, part, jax.ShapeDtypeStruct((3, gate.shape[1], count), BF)],
        compiler_params=params(24),
        name="forward",
    )(core, own, other, gate, up, down)


def grads_kernel(core_s, delta_ref, own_ref, other_ref, gate_ref, up_ref, down_ref, norm_ref):
    core = core_s[0]
    step = 2 * LANES
    norms = []
    for k, (out, which) in enumerate(((gate_ref, 0), (up_ref, 0), (down_ref, 1))):
        total = 0.0
        for side, ref in ((core, own_ref), (1 - core, other_ref)):
            for s in range(0, HALF, step):
                g = dot(delta_ref[k], ref[which, :, s : s + step])
                cols = pl.ds(pl.multiple_of(side * HALF + s, step), step)
                out[0, :, cols] = g.astype(BF)
                sq = g * g
                total = total + sq[:, :LANES] + sq[:, LANES:]
        norms.append(jnp.sum(total.T, axis=0, keepdims=True))
    norm_ref[...] = jnp.concatenate(norms, axis=0)


def grads(core, delta, own, other):
    feats = delta.shape[1]
    out = jax.ShapeDtypeStruct((1, feats, 2 * HALF), BF)
    return pl.pallas_call(
        grads_kernel,
        in_specs=in_smem(1) + in_vmem(3),
        out_specs=in_vmem(4),
        out_shape=[out, out, out, jax.ShapeDtypeStruct((3, feats), F32)],
        compiler_params=params(24),
        name="grads",
    )(core, delta, own, other)


def back_kernel(cap, keep_ref, take_ref, norm_ref, out_ref, tiles):
    n = out_ref.shape[0]
    count = n * cap
    for j in range(TILE):
        cols = slice(j * LANES, (j + 1) * LANES)
        both = keep_ref[:count, cols].astype(F32) + take_ref[:count, cols].astype(F32)
        tiles[pl.ds(j, count, stride=TILE), :] = both
    out_ref[:, :cap] = tiles[...].astype(BF).reshape(n, cap, TILE, LANES)
    both = keep_ref[count:, :LANES].astype(F32) + take_ref[count:, :LANES].astype(F32)
    lines = -(-count // LANES)
    hi, lo = split2(both[:lines] + both[lines : 2 * lines])
    norm_hi, norm_lo = split2(norm_ref[:1])
    norm = jnp.where(iota((1, LANES), 1) < LANES // 2, norm_hi, norm_lo)
    pad = jnp.zeros((TILE - 2 * lines - 1, LANES), F32)
    tile = jnp.concatenate([hi, lo, norm, pad], axis=0).astype(BF)
    out_ref[:, cap] = jnp.broadcast_to(tile[None], (n, TILE, LANES))


def back_rows(keep, take, norms, n, cap):
    return pl.pallas_call(
        functools.partial(back_kernel, cap),
        in_specs=in_vmem(3),
        out_specs=pl.BlockSpec(memory_space=pltpu.VMEM),
        out_shape=jax.ShapeDtypeStruct((n, cap + 1, TILE, LANES), BF),
        scratch_shapes=[pltpu.VMEM((n * cap * TILE, LANES), F32)],
        compiler_params=params(16),
        name="back_rows",
    )(keep, take, norms)


def combine_kernel(cap, ids_s, rank_s, me_s, recv_ref, ids_ref, rank_ref, out_ref, norm_ref, tiles):
    n = recv_ref.shape[0]
    count = ids_ref.shape[1]

    def one_token(t, carry):
        pair = [recv_ref[ids_s[k, t], rank_s[k, t]].astype(F32) for k in range(2)]
        tiles[pl.ds(pl.multiple_of(t * TILE, TILE), TILE), :] = pair[0] + pair[1]
        return carry

    lax.fori_loop(0, count, one_token, 0, unroll=8)
    for j in range(TILE):
        out_ref[j, :count] = gather_cols(tiles, count, j).astype(BF)
    extra = recv_ref[:, cap].reshape(n * TILE, LANES)
    lines = -(-n * cap // LANES)
    o = iota((n * TILE, count), 0)
    route = []
    for k in range(2):
        slot = me_s[0] * cap + rank_ref[k : k + 1, :]
        first = ids_ref[k : k + 1, :] * TILE + slot // LANES
        got = dot(extra, ones_at((o == first) | (o == first + lines)), 0, 0)
        use = iota((LANES, count), 0) == slot % LANES
        route.append(jnp.sum(jnp.where(use, got, 0.0), axis=0, keepdims=True))
    hi, lo = split2(jnp.concatenate(route, axis=0))
    tile = jnp.concatenate([hi, lo, jnp.zeros((TILE - 4, count), F32)], axis=0).astype(BF)
    out_ref[:, count:] = jnp.broadcast_to(tile[None], (TILE, TILE, LANES))
    sums = dot(ones_at(iota((TILE, n * TILE), 1) % TILE == 2 * lines), extra)
    norm_ref[...] = sums[:, : LANES // 2] + sums[:, LANES // 2 :]


def combine(ids_t, rank, me, recv, cap):
    count = ids_t.shape[1]
    return pl.pallas_call(
        functools.partial(combine_kernel, cap),
        in_specs=in_smem(3) + in_vmem(3),
        out_specs=in_vmem(2),
        out_shape=[
            jax.ShapeDtypeStruct((TILE, count + TILE, LANES), BF),
            jax.ShapeDtypeStruct((TILE, LANES // 2), F32),
        ],
        scratch_shapes=[pltpu.VMEM((count * TILE, LANES), F32)],
        compiler_params=params(16),
        name="combine",
    )(ids_t, rank, me, recv, ids_t, rank)


def end_kernel(recv_ref, w_ref, tok_ref, route_ref):
    count = tok_ref.shape[0]
    total = recv_ref[0].astype(F32)
    for x in range(1, recv_ref.shape[0]):
        total = total + recv_ref[x].astype(F32)
    tok_ref[...] = total[:count].astype(BF)
    route_ref[...] = (total[count : count + 2] + total[count + 2 : count + 4]) / w_ref[...]


def end(recv, w_t):
    count = w_t.shape[1]
    return pl.pallas_call(
        end_kernel,
        in_specs=in_vmem(2),
        out_specs=in_vmem(2),
        out_shape=[
            jax.ShapeDtypeStruct((count, LANES), BF),
            jax.ShapeDtypeStruct((2, count), F32),
        ],
        compiler_params=params(16),
        name="end",
    )(recv, w_t)


def swap(v):
    return lax.ppermute(v, "c", [(0, 1), (1, 0)])


def local(tokens, out_grad, expert_ids, route_weights, gate_proj, up_proj, down_proj, shared_act):
    n = lax.axis_size(EP)
    cap = 5 * tokens.shape[0] * expert_ids.shape[1] // (4 * n)
    core = lax.axis_index("c").reshape(1)
    at = lax.axis_index(TP).reshape(1)
    me = lax.axis_index(EP).reshape(1)
    ids_t, w_t = expert_ids.T, route_weights.T
    sent, rank = send_rows(ids_t, w_t, at, tokens, out_grad, shared_act, cap, n)
    recv = lax.all_to_all(sent, EP, 0, 0, tiled=True)
    own = unpack(recv, cap)
    other = swap(own)
    shared, norms = shared_sum(recv, cap)
    keep, give, delta = forward(core, own, other, gate_proj, up_proj, down_proj)
    back = back_rows(keep, swap(give), norms, n, cap)
    returned = lax.all_to_all(back, EP, 0, 0, tiled=True)
    gate_grad, up_grad, down_grad, row_norms = grads(core, delta, own, other)
    parts, shared_norms = combine(ids_t, rank, me, returned, cap)
    summed = lax.all_to_all(parts, "x", 0, 0, tiled=True)
    token_grad, route_grad = end(summed, w_t)
    return (
        token_grad,
        route_grad.T,
        gate_grad,
        up_grad,
        down_grad,
        row_norms[None],
        shared.T,
        shared_norms[0],
    )


def solution(mesh):
    torus = Mesh(mesh.devices.reshape(8, 8, mesh.shape["tp"] // 2, 2), (*EP, *TP))
    return jax.shard_map(
        local,
        mesh=torus,
        in_specs=(
            P(EP, None),
            P(EP, None),
            P(EP, None),
            P(EP, None),
            P(EP, TP, None),
            P(EP, TP, None),
            P(EP, TP, None),
            P(EP, None),
        ),
        out_specs=(
            P(EP, TP),
            P(EP, None),
            P(EP, TP, None),
            P(EP, TP, None),
            P(EP, TP, None),
            P(EP, None, TP),
            P(TP, EP),
            P(TP),
        ),
        check_vma=False,
    )
```

```python
import functools

import jax
import jax.numpy as jnp
from jax import lax
from jax.experimental import pallas as pl
from jax.experimental.pallas import tpu as pltpu
from jax.sharding import Mesh
from jax.sharding import PartitionSpec as P

EP = ("z", "y")
TP = ("x", "c")
BF, F32, I32 = jnp.bfloat16, jnp.float32, jnp.int32
LANES = 128
TILE = 8
HALF = TILE * LANES
SHARED = 2
GROUP = 16


def params(mib):
    return pltpu.CompilerParams(vmem_limit_bytes=mib * 1024 * 1024)


def in_vmem(n):
    return [pl.BlockSpec(memory_space=pltpu.VMEM)] * n


def in_smem(n):
    return [pl.BlockSpec(memory_space=pltpu.SMEM)] * n


def iota(shape, dim):
    return lax.broadcasted_iota(I32, shape, dim)


def ones_at(mask):
    return mask.astype(F32).astype(BF)


def dot(a, b, ca=1, cb=0):
    return lax.dot_general(a, b, (((ca,), (cb,)), ((), ())), preferred_element_type=F32)


def split2(v):
    hi = v.astype(BF).astype(F32)
    return hi, v - hi


def spread(ref, x):
    for j in range(TILE):
        cols = x[:, j * LANES : (j + 1) * LANES].astype(F32)
        ref[pl.ds(j, x.shape[0], stride=TILE), :] = cols


def gather_cols(ref, count, j):
    return ref[pl.ds(j, count, stride=TILE), :]


def send_kernel(
    cap, at_s, me_s, tok_ref, grad_ref, act_ref, ids_ref, w_ref, out_ref, rank_s,
    tok_v, grad_v, act_v, ids_s, w_s, seen_s, tok_t, grad_t, sems,
):
    del me_s
    count, width = grad_ref.shape
    experts = out_ref.shape[0]
    mine = pl.ds(pl.multiple_of((at_s[0] % 2) * HALF, HALF), HALF)
    line = pl.ds(pl.multiple_of((at_s[0] // 2) * LANES, LANES), LANES)
    pairs = (
        (act_ref.at[:, line], act_v),
        (grad_ref, grad_v),
        (tok_ref.at[:, mine], tok_v),
        (ids_ref, ids_s),
        (w_ref, w_s),
    )
    copies = [pltpu.make_async_copy(a, b, sems.at[i]) for i, (a, b) in enumerate(pairs)]
    for c in copies:
        c.start()
    for e in range(experts):
        seen_s[e] = 0
    out_ref[:, : 2 * cap] = jnp.zeros((experts, 2 * cap, TILE, LANES), BF)
    for c in copies:
        c.wait()
    spread(tok_t, tok_v[...])
    spread(grad_t, grad_v[:, mine])

    def one_token(t, carry):
        rows = pl.ds(pl.multiple_of(t * TILE, TILE), TILE)
        tok = tok_t[rows, :].astype(BF)
        grad = grad_t[rows, :]
        for k in range(2):
            e = ids_s[k, t]
            r = seen_s[e]
            seen_s[e] = r + 1
            rank_s[k, t] = r
            out_ref[e, r] = tok
            out_ref[e, cap + r] = (w_s[k, t] * grad).astype(BF)
        return carry

    lax.fori_loop(0, count, one_token, 0, unroll=8)

    half = LANES // 2
    act = act_v[...]
    swapped = jnp.concatenate([act[:, half:], act[:, :half]], axis=1)
    own = (at_s[0] % 2) * half
    keep = (iota(act.shape, 1) // half) * half == own
    twice = jnp.where(keep, act.astype(F32), swapped.astype(F32)).astype(BF)
    step = 2 * LANES
    block = width // experts
    for s in range(0, width, step):
        term = dot(grad_v[:, s : s + step], twice, 0, 0)
        term = term.reshape(step // block, 2, block // 2, LANES)
        lane = iota((step // block, block // 2, LANES), 2)
        both = jnp.where(lane < half, term[:, 0], term[:, 1]).astype(BF)
        out_ref[s // block : (s + step) // block, 2 * cap :] = both.reshape(
            step // block, SHARED, TILE, LANES
        )


def send_rows(at, me, tokens, out_grad, act, ids_t, w_t, cap, experts):
    count, width = out_grad.shape
    return pl.pallas_call(
        functools.partial(send_kernel, cap),
        in_specs=in_smem(2) + [pl.BlockSpec(memory_space=pltpu.HBM)] * 5,
        out_specs=in_vmem(1) + in_smem(1),
        out_shape=[
            jax.ShapeDtypeStruct((experts, 2 * cap + SHARED, TILE, LANES), BF),
            jax.ShapeDtypeStruct((2, count), I32),
        ],
        scratch_shapes=[
            pltpu.VMEM((count, HALF), BF),
            pltpu.VMEM((count, width), BF),
            pltpu.VMEM((count, LANES), BF),
            pltpu.SMEM((2, count), I32),
            pltpu.SMEM((2, count), F32),
            pltpu.SMEM((experts,), I32),
            pltpu.VMEM((count * TILE, LANES), F32),
            pltpu.VMEM((count * TILE, LANES), F32),
            pltpu.SemaphoreType.DMA((5,)),
        ],
        compiler_params=params(16),
        name="send_rows",
    )(at, me, tokens, out_grad, act, ids_t, w_t)


def shared_kernel(cap, recv_ref, out_ref, norm_ref):
    total = jnp.sum(recv_ref[:, 2 * cap :].astype(F32), axis=0).reshape(SHARED * TILE, LANES)
    half = LANES // 2
    out_ref[...] = jnp.concatenate([total[:, :half], total[:, half:]], axis=0)
    sq = jnp.sum(total * total, axis=0, keepdims=True)
    sq = sq + jnp.concatenate([sq[:, half:], sq[:, :half]], axis=1)
    norm_ref[...] = jnp.broadcast_to(sq, norm_ref.shape)


def shared_sum(recv, cap):
    return pl.pallas_call(
        functools.partial(shared_kernel, cap),
        in_specs=in_vmem(1),
        out_specs=in_vmem(2),
        out_shape=[
            jax.ShapeDtypeStruct((32, LANES // 2), F32),
            jax.ShapeDtypeStruct((TILE, LANES), F32),
        ],
        compiler_params=params(16),
        name="shared_sum",
    )(recv)


def unpack_kernel(cap, recv_ref, rows_ref, in_t, cot_t):
    n = recv_ref.shape[0]
    count = n * cap
    for k, ref in enumerate((in_t, cot_t)):
        tiles = recv_ref[:, k * cap : (k + 1) * cap].astype(F32)
        ref[...] = tiles.reshape(count * TILE, LANES)
        for j in range(TILE):
            cols = slice(j * LANES, (j + 1) * LANES)
            rows_ref[k, :, cols] = gather_cols(ref, count, j).astype(BF)


def unpack(recv, cap):
    count = recv.shape[0] * cap
    return pl.pallas_call(
        functools.partial(unpack_kernel, cap),
        in_specs=in_vmem(1),
        out_specs=pl.BlockSpec(memory_space=pltpu.VMEM),
        out_shape=jax.ShapeDtypeStruct((2, count, HALF), BF),
        scratch_shapes=[pltpu.VMEM((count * TILE, LANES), F32)] * 2,
        compiler_params=params(16),
        name="unpack",
    )(recv)


def products(side, rows_ref, gate_ref, up_ref, down_ref, sums):
    step = 2 * LANES
    for s in range(0, HALF, step):
        cols = pl.ds(pl.multiple_of(side * HALF + s, step), step)
        a, b = rows_ref[0, :, s : s + step], rows_ref[1, :, s : s + step]
        for k, (x, w) in enumerate(((a, gate_ref), (a, up_ref), (b, down_ref))):
            sums[k] = sums[k] + dot(x, w[0, :, cols], 1, 1)
    return sums


def half_kernel(core_s, own_ref, gate_ref, up_ref, down_ref, out_ref):
    sums = products(core_s[0], own_ref, gate_ref, up_ref, down_ref, [0.0] * 3)
    for k in range(3):
        out_ref[k] = sums[k]


def half_products(core, own, gate, up, down):
    return pl.pallas_call(
        half_kernel,
        in_specs=in_smem(1) + in_vmem(4),
        out_specs=pl.BlockSpec(memory_space=pltpu.VMEM),
        out_shape=jax.ShapeDtypeStruct((3, own.shape[1], gate.shape[1]), F32),
        compiler_params=params(16),
        name="half_products",
    )(core, own, gate, up, down)


def shares(side, deltas, gate_ref, up_ref, inner, ref):
    count = deltas.shape[0]
    for j in range(ref.shape[0]):
        cols = pl.ds(pl.multiple_of(j * 2 * LANES + side * LANES, LANES), LANES)
        w = jnp.concatenate([gate_ref[0, :, cols], up_ref[0, :, cols]], axis=0)
        ref[j, :count] = dot(deltas, w).astype(BF)
        ref[j, count:] = inner


def forward_kernel(
    cap, core_s, half_ref, other_ref, gate_ref, up_ref, down_ref, give_ref, delta_ref, inner_ref
):
    core = core_s[0]
    count = other_ref.shape[1]
    sums = products(1 - core, other_ref, gate_ref, up_ref, down_ref, [half_ref[k] for k in range(3)])
    gate_pre, up_pre, hidden_grad = sums
    sig = jax.nn.sigmoid(gate_pre)
    silu = gate_pre * sig
    hidden = (silu * up_pre).astype(BF)
    up_delta = (hidden_grad * silu).astype(BF)
    gate_delta = (hidden_grad * up_pre * sig * (1.0 + gate_pre * (1.0 - sig))).astype(BF)
    inner = jnp.sum(hidden.astype(F32) * hidden_grad, axis=1, keepdims=True)
    slot = iota((count, LANES), 0)
    lane = (slot // cap) % GROUP * TILE + slot % cap
    spots = jnp.where(lane == iota((count, LANES), 1), inner, 0.0)
    span = GROUP * cap
    lines = [jnp.sum(spots[s : s + span], axis=0, keepdims=True) for s in range(0, count, span)]
    tile = jnp.concatenate(split2(jnp.concatenate(lines, axis=0)), axis=0).astype(BF)
    inner_ref[...] = tile
    shares(1 - core, jnp.concatenate([gate_delta, up_delta], axis=1), gate_ref, up_ref, tile, give_ref)
    for k, d in enumerate((gate_delta, up_delta, hidden)):
        delta_ref[k] = d


def forward(core, half, other, gate, up, down, cap):
    count = other.shape[1]
    return pl.pallas_call(
        functools.partial(forward_kernel, cap),
        in_specs=in_smem(1) + in_vmem(5),
        out_specs=in_vmem(3),
        out_shape=[
            jax.ShapeDtypeStruct((TILE, count + TILE, LANES), BF),
            jax.ShapeDtypeStruct((3, count, gate.shape[1]), BF),
            jax.ShapeDtypeStruct((TILE, LANES), BF),
        ],
        compiler_params=params(24),
        name="forward",
    )(core, half, other, gate, up, down)


def keep_kernel(core_s, delta_ref, inner_ref, gate_ref, up_ref, keep_ref):
    deltas = jnp.concatenate([delta_ref[0], delta_ref[1]], axis=1)
    shares(core_s[0], deltas, gate_ref, up_ref, inner_ref[...], keep_ref)


def keep_shares(core, delta, inner, gate, up):
    return pl.pallas_call(
        keep_kernel,
        in_specs=in_smem(1) + in_vmem(4),
        out_specs=pl.BlockSpec(memory_space=pltpu.VMEM),
        out_shape=jax.ShapeDtypeStruct((TILE, delta.shape[1] + TILE, LANES), BF),
        compiler_params=params(16),
        name="keep_shares",
    )(core, delta, inner, gate, up)


def pair_kernel(a_ref, b_ref, out_ref):
    out_ref[...] = (a_ref[...].astype(F32) + b_ref[...].astype(F32)).astype(BF)


def pair_sum(a, b):
    return pl.pallas_call(
        pair_kernel,
        in_specs=in_vmem(2),
        out_specs=pl.BlockSpec(memory_space=pltpu.VMEM),
        out_shape=jax.ShapeDtypeStruct(a.shape, BF),
        compiler_params=params(16),
        name="pair_sum",
    )(a, b)


def grads_kernel(core_s, delta_ref, own_ref, other_ref, gate_ref, up_ref, down_ref, norm_ref):
    core = core_s[0]
    step = 2 * LANES
    for k, (out, which) in enumerate(((gate_ref, 0), (up_ref, 0), (down_ref, 1))):
        total = 0.0
        delta = delta_ref[k].astype(F32).T.astype(BF)
        for side, ref in ((core, own_ref), (1 - core, other_ref)):
            for s in range(0, HALF, step):
                g = dot(delta, ref[which, :, s : s + step])
                cols = pl.ds(pl.multiple_of(side * HALF + s, step), step)
                out[0, :, cols] = g.astype(BF)
                sq = g * g
                total = total + sq[:, :LANES] + sq[:, LANES:]
        norm_ref[k] = jnp.sum(total.T, axis=0, keepdims=True)


def grads(core, delta, own, other):
    feats = delta.shape[2]
    out = jax.ShapeDtypeStruct((1, feats, 2 * HALF), BF)
    return pl.pallas_call(
        grads_kernel,
        in_specs=in_smem(1) + in_vmem(3),
        out_specs=in_vmem(4),
        out_shape=[out, out, out, jax.ShapeDtypeStruct((3, 1, feats), F32)],
        compiler_params=params(24),
        name="grads",
    )(core, delta, own, other)


def back_kernel(cap, parts_ref, norm_ref, out_ref, sums, rows):
    n = out_ref.shape[0]
    count = n * cap
    total = parts_ref[0].astype(F32)
    for x in range(1, parts_ref.shape[0]):
        total = total + parts_ref[x].astype(F32)
    sums[...] = total
    for r in range(cap):
        rows[pl.ds(r, n, stride=TILE), :] = sums[pl.ds(r, n, stride=cap), :]
    lines = n // GROUP
    inner = split2(total[count : count + lines] + total[count + lines : count + 2 * lines])
    for r, part in zip((cap, cap + 2), inner):
        spread_lines = [
            jnp.broadcast_to(part[g : g + 1], (GROUP, LANES)) for g in range(lines)
        ]
        rows[pl.ds(r, n, stride=TILE), :] = jnp.concatenate(spread_lines, axis=0)
    norm_hi, norm_lo = split2(norm_ref[:1])
    norm = jnp.where(iota((1, LANES), 1) < LANES // 2, norm_hi, norm_lo)
    rows[pl.ds(cap + 1, n, stride=TILE), :] = jnp.broadcast_to(norm, (n, LANES))
    out_ref[...] = rows[...].astype(BF).reshape(n, TILE, LANES)


def back_rows(parts, norms, n, cap):
    return pl.pallas_call(
        functools.partial(back_kernel, cap),
        in_specs=in_vmem(2),
        out_specs=pl.BlockSpec(memory_space=pltpu.VMEM),
        out_shape=jax.ShapeDtypeStruct((n, TILE, LANES), BF),
        scratch_shapes=[
            pltpu.VMEM(parts.shape[1:], F32),
            pltpu.VMEM((n * TILE, LANES), F32),
        ],
        compiler_params=params(16),
        name="back_rows",
    )(parts, norms)


def end_kernel(cap, me_s, recv_ref, ids_ref, rank_ref, w_ref, tok_ref, route_ref, norm_ref):
    n = recv_ref.shape[0]
    count = ids_ref.shape[1]
    rows = recv_ref[...].reshape(n * TILE, LANES)
    o = iota((n * TILE, count), 0)
    first = [ids_ref[k : k + 1, :] * TILE for k in range(2)]
    rank = [rank_ref[k : k + 1, :] for k in range(2)]
    pick = ones_at((o == first[0] + rank[0]) | (o == first[1] + rank[1]))
    tok_ref[...] = dot(pick, rows, 0, 0).astype(BF)
    route = []
    for k in range(2):
        pick = ones_at((o == first[k] + cap) | (o == first[k] + cap + 2))
        got = dot(rows, pick, 0, 0)
        use = iota((LANES, count), 0) == (me_s[0] % GROUP) * TILE + rank[k]
        route.append(jnp.sum(jnp.where(use, got, 0.0), axis=0, keepdims=True))
    route_ref[...] = jnp.concatenate(route, axis=0) / w_ref[...]
    sums = dot(ones_at(iota((TILE, n * TILE), 1) % TILE == cap + 1), rows)
    norm_ref[...] = sums[:1, : LANES // 2] + sums[:1, LANES // 2 :]


def end(me, recv, ids_t, rank, w_t, cap):
    count = ids_t.shape[1]
    return pl.pallas_call(
        functools.partial(end_kernel, cap),
        in_specs=in_smem(1) + in_vmem(4),
        out_specs=in_vmem(3),
        out_shape=[
            jax.ShapeDtypeStruct((count, LANES), BF),
            jax.ShapeDtypeStruct((2, count), F32),
            jax.ShapeDtypeStruct((1, LANES // 2), F32),
        ],
        compiler_params=params(16),
        name="end",
    )(me, recv, ids_t, rank, w_t)


def swap(v):
    return lax.ppermute(v, "c", [(0, 1), (1, 0)])


def local(tokens, out_grad, expert_ids, route_weights, gate_proj, up_proj, down_proj, shared_act):
    n = lax.axis_size(EP)
    cap = 5 * tokens.shape[0] * expert_ids.shape[1] // (4 * n)
    core = lax.axis_index("c").reshape(1)
    at = lax.axis_index(TP).reshape(1)
    me = lax.axis_index(EP).reshape(1)
    ids_t, w_t = expert_ids.T, route_weights.T
    here = (tokens, out_grad, shared_act, ids_t, w_t)
    here = [pltpu.with_memory_space_constraint(v, pltpu.HBM) for v in here]
    sent, rank = send_rows(at, me, *here, cap, n)
    recv = lax.all_to_all(sent, EP, 0, 0, tiled=True)
    own = unpack(recv, cap)
    other = swap(own)
    half = half_products(core, own, gate_proj, up_proj, down_proj)
    shared, norms = shared_sum(recv, cap)
    give, delta, inner = forward(core, half, other, gate_proj, up_proj, down_proj, cap)
    take = swap(give)
    keep = keep_shares(core, delta, inner, gate_proj, up_proj)
    parts = lax.all_to_all(pair_sum(keep, take), "x", 0, 0, tiled=True)
    gate_grad, up_grad, down_grad, row_norms = grads(core, delta, own, other)
    back = back_rows(parts, norms, n, cap)
    returned = lax.all_to_all(back, EP, 0, 0, tiled=True)
    token_grad, route_grad, shared_norms = end(me, returned, ids_t, rank, w_t, cap)
    return (
        token_grad,
        route_grad.T,
        gate_grad,
        up_grad,
        down_grad,
        row_norms.transpose(1, 0, 2),
        shared.T,
        shared_norms.reshape(-1),
    )


def solution(mesh):
    torus = Mesh(mesh.devices.reshape(8, 8, mesh.shape["tp"] // 2, 2), (*EP, *TP))
    return jax.shard_map(
        local,
        mesh=torus,
        in_specs=(
            P(EP, None),
            P(EP, None),
            P(EP, None),
            P(EP, None),
            P(EP, TP, None),
            P(EP, TP, None),
            P(EP, TP, None),
            P(EP, None),
        ),
        out_specs=(
            P(EP, TP),
            P(EP, None),
            P(EP, TP, None),
            P(EP, TP, None),
            P(EP, TP, None),
            P(EP, None, TP),
            P(TP, EP),
            P(TP),
        ),
        check_vma=False,
    )
```

```python
import functools

import jax
import jax.numpy as jnp
from jax import lax
from jax.experimental import pallas as pl
from jax.experimental.pallas import tpu as pltpu
from jax.sharding import Mesh
from jax.sharding import PartitionSpec as P

EP = ("z", "y")
TP = ("x", "c")
BF, F32, I32 = jnp.bfloat16, jnp.float32, jnp.int32
LANES = 128
TILE = 8
HALF = TILE * LANES
SHARED = 2
GROUP = 16


def params(mib):
    return pltpu.CompilerParams(vmem_limit_bytes=mib * 1024 * 1024)


def in_vmem(n):
    return [pl.BlockSpec(memory_space=pltpu.VMEM)] * n


def in_smem(n):
    return [pl.BlockSpec(memory_space=pltpu.SMEM)] * n


def iota(shape, dim):
    return lax.broadcasted_iota(I32, shape, dim)


def ones_at(mask):
    return mask.astype(F32).astype(BF)


def dot(a, b, ca=1, cb=0):
    return lax.dot_general(a, b, (((ca,), (cb,)), ((), ())), preferred_element_type=F32)


def split2(v):
    hi = v.astype(BF).astype(F32)
    return hi, v - hi


def spread(ref, x):
    for j in range(TILE):
        cols = x[:, j * LANES : (j + 1) * LANES].astype(F32)
        ref[pl.ds(j, x.shape[0], stride=TILE), :] = cols


def gather_cols(ref, count, j):
    return ref[pl.ds(j, count, stride=TILE), :]


def send_kernel(
    cap, at_s, me_s, tok_ref, grad_ref, act_ref, ids_ref, w_ref, out_ref, rank_s,
    tok_v, grad_v, act_v, ids_s, w_s, seen_s, tok_t, grad_t, sems,
):
    del me_s
    count, width = grad_ref.shape
    experts = out_ref.shape[0]
    mine = pl.ds(pl.multiple_of((at_s[0] % 2) * HALF, HALF), HALF)
    line = pl.ds(pl.multiple_of((at_s[0] // 2) * LANES, LANES), LANES)
    pairs = (
        (act_ref.at[:, line], act_v),
        (grad_ref, grad_v),
        (tok_ref.at[:, mine], tok_v),
        (ids_ref, ids_s),
        (w_ref, w_s),
    )
    copies = [pltpu.make_async_copy(a, b, sems.at[i]) for i, (a, b) in enumerate(pairs)]
    for c in copies:
        c.start()
    for e in range(experts):
        seen_s[e] = 0
    out_ref[:, : 2 * cap] = jnp.zeros((experts, 2 * cap, TILE, LANES), BF)
    for c in copies:
        c.wait()
    spread(tok_t, tok_v[...])
    spread(grad_t, grad_v[:, mine])

    def one_token(t, carry):
        rows = pl.ds(pl.multiple_of(t * TILE, TILE), TILE)
        tok = tok_t[rows, :].astype(BF)
        grad = grad_t[rows, :]
        for k in range(2):
            e = ids_s[k, t]
            r = seen_s[e]
            seen_s[e] = r + 1
            rank_s[k, t] = r
            out_ref[e, r] = tok
            out_ref[e, cap + r] = (w_s[k, t] * grad).astype(BF)
        return carry

    lax.fori_loop(0, count, one_token, 0, unroll=8)

    half = LANES // 2
    act = act_v[...]
    swapped = jnp.concatenate([act[:, half:], act[:, :half]], axis=1)
    own = (at_s[0] % 2) * half
    keep = (iota(act.shape, 1) // half) * half == own
    twice = jnp.where(keep, act.astype(F32), swapped.astype(F32)).astype(BF)
    step = 2 * LANES
    block = width // experts
    for s in range(0, width, step):
        term = dot(grad_v[:, s : s + step], twice, 0, 0)
        term = term.reshape(step // block, 2, block // 2, LANES)
        lane = iota((step // block, block // 2, LANES), 2)
        both = jnp.where(lane < half, term[:, 0], term[:, 1]).astype(BF)
        out_ref[s // block : (s + step) // block, 2 * cap :] = both.reshape(
            step // block, SHARED, TILE, LANES
        )


def send_rows(at, me, tokens, out_grad, act, ids_t, w_t, cap, experts):
    count, width = out_grad.shape
    return pl.pallas_call(
        functools.partial(send_kernel, cap),
        in_specs=in_smem(2) + [pl.BlockSpec(memory_space=pltpu.HBM)] * 5,
        out_specs=in_vmem(1) + in_smem(1),
        out_shape=[
            jax.ShapeDtypeStruct((experts, 2 * cap + SHARED, TILE, LANES), BF),
            jax.ShapeDtypeStruct((2, count), I32),
        ],
        scratch_shapes=[
            pltpu.VMEM((count, HALF), BF),
            pltpu.VMEM((count, width), BF),
            pltpu.VMEM((count, LANES), BF),
            pltpu.SMEM((2, count), I32),
            pltpu.SMEM((2, count), F32),
            pltpu.SMEM((experts,), I32),
            pltpu.VMEM((count * TILE, LANES), F32),
            pltpu.VMEM((count * TILE, LANES), F32),
            pltpu.SemaphoreType.DMA((5,)),
        ],
        compiler_params=params(16),
        name="send_rows",
    )(at, me, tokens, out_grad, act, ids_t, w_t)


def shared_kernel(cap, recv_ref, out_ref, norm_ref):
    total = jnp.sum(recv_ref[:, 2 * cap :].astype(F32), axis=0).reshape(SHARED * TILE, LANES)
    half = LANES // 2
    out_ref[...] = jnp.concatenate([total[:, :half], total[:, half:]], axis=0)
    sq = jnp.sum(total * total, axis=0, keepdims=True)
    sq = sq + jnp.concatenate([sq[:, half:], sq[:, :half]], axis=1)
    norm_ref[...] = jnp.broadcast_to(sq, norm_ref.shape)


def shared_sum(recv, cap):
    return pl.pallas_call(
        functools.partial(shared_kernel, cap),
        in_specs=in_vmem(1),
        out_specs=in_vmem(2),
        out_shape=[
            jax.ShapeDtypeStruct((32, LANES // 2), F32),
            jax.ShapeDtypeStruct((TILE, LANES), F32),
        ],
        compiler_params=params(16),
        name="shared_sum",
    )(recv)


def unpack_kernel(cap, recv_ref, rows_ref, in_t, cot_t):
    n = recv_ref.shape[0]
    count = n * cap
    for k, ref in enumerate((in_t, cot_t)):
        tiles = recv_ref[:, k * cap : (k + 1) * cap].astype(F32)
        ref[...] = tiles.reshape(count * TILE, LANES)
        for j in range(TILE):
            cols = slice(j * LANES, (j + 1) * LANES)
            rows_ref[k, :, cols] = gather_cols(ref, count, j).astype(BF)


def unpack(recv, cap):
    count = recv.shape[0] * cap
    return pl.pallas_call(
        functools.partial(unpack_kernel, cap),
        in_specs=in_vmem(1),
        out_specs=pl.BlockSpec(memory_space=pltpu.VMEM),
        out_shape=jax.ShapeDtypeStruct((2, count, HALF), BF),
        scratch_shapes=[pltpu.VMEM((count * TILE, LANES), F32)] * 2,
        compiler_params=params(16),
        name="unpack",
    )(recv)


def products(side, rows_ref, gate_ref, up_ref, down_ref, sums):
    step = 2 * LANES
    for s in range(0, HALF, step):
        cols = pl.ds(pl.multiple_of(side * HALF + s, step), step)
        a, b = rows_ref[0, :, s : s + step], rows_ref[1, :, s : s + step]
        for k, (x, w) in enumerate(((a, gate_ref), (a, up_ref), (b, down_ref))):
            sums[k] = sums[k] + dot(x, w[0, :, cols], 1, 1)
    return sums


def half_kernel(core_s, own_ref, gate_ref, up_ref, down_ref, out_ref):
    sums = products(core_s[0], own_ref, gate_ref, up_ref, down_ref, [0.0] * 3)
    for k in range(3):
        out_ref[k] = sums[k]


def half_products(core, own, gate, up, down):
    return pl.pallas_call(
        half_kernel,
        in_specs=in_smem(1) + in_vmem(4),
        out_specs=pl.BlockSpec(memory_space=pltpu.VMEM),
        out_shape=jax.ShapeDtypeStruct((3, own.shape[1], gate.shape[1]), F32),
        compiler_params=params(16),
        name="half_products",
    )(core, own, gate, up, down)


def shares(side, deltas, gate_ref, up_ref, inner, ref):
    count = deltas.shape[0]
    for j in range(ref.shape[0]):
        cols = pl.ds(pl.multiple_of(j * 2 * LANES + side * LANES, LANES), LANES)
        w = jnp.concatenate([gate_ref[0, :, cols], up_ref[0, :, cols]], axis=0)
        ref[j, :count] = dot(deltas, w).astype(BF)
        ref[j, count:] = inner


def forward_kernel(
    cap, core_s, half_ref, other_ref, gate_ref, up_ref, down_ref, give_ref, delta_ref, inner_ref
):
    core = core_s[0]
    count = other_ref.shape[1]
    sums = products(1 - core, other_ref, gate_ref, up_ref, down_ref, [half_ref[k] for k in range(3)])
    gate_pre, up_pre, hidden_grad = sums
    sig = jax.nn.sigmoid(gate_pre)
    silu = gate_pre * sig
    hidden = (silu * up_pre).astype(BF)
    up_delta = (hidden_grad * silu).astype(BF)
    gate_delta = (hidden_grad * up_pre * sig * (1.0 + gate_pre * (1.0 - sig))).astype(BF)
    inner = jnp.sum(hidden.astype(F32) * hidden_grad, axis=1, keepdims=True)
    slot = iota((count, LANES), 0)
    lane = (slot // cap) % GROUP * TILE + slot % cap
    spots = jnp.where(lane == iota((count, LANES), 1), inner, 0.0)
    span = GROUP * cap
    lines = [jnp.sum(spots[s : s + span], axis=0, keepdims=True) for s in range(0, count, span)]
    tile = jnp.concatenate(split2(jnp.concatenate(lines, axis=0)), axis=0).astype(BF)
    inner_ref[...] = tile
    shares(1 - core, jnp.concatenate([gate_delta, up_delta], axis=1), gate_ref, up_ref, tile, give_ref)
    for k, d in enumerate((gate_delta, up_delta, hidden)):
        delta_ref[k] = d


def forward(core, half, other, gate, up, down, cap):
    count = other.shape[1]
    return pl.pallas_call(
        functools.partial(forward_kernel, cap),
        in_specs=in_smem(1) + in_vmem(5),
        out_specs=in_vmem(3),
        out_shape=[
            jax.ShapeDtypeStruct((TILE, count + TILE, LANES), BF),
            jax.ShapeDtypeStruct((3, count, gate.shape[1]), BF),
            jax.ShapeDtypeStruct((TILE, LANES), BF),
        ],
        compiler_params=params(24),
        name="forward",
    )(core, half, other, gate, up, down)


def keep_kernel(core_s, delta_ref, inner_ref, gate_ref, up_ref, keep_ref):
    deltas = jnp.concatenate([delta_ref[0], delta_ref[1]], axis=1)
    shares(core_s[0], deltas, gate_ref, up_ref, inner_ref[...], keep_ref)


def keep_shares(core, delta, inner, gate, up):
    return pl.pallas_call(
        keep_kernel,
        in_specs=in_smem(1) + in_vmem(4),
        out_specs=pl.BlockSpec(memory_space=pltpu.VMEM),
        out_shape=jax.ShapeDtypeStruct((TILE, delta.shape[1] + TILE, LANES), BF),
        compiler_params=params(16),
        name="keep_shares",
    )(core, delta, inner, gate, up)


def back_kernel(cap, keep_ref, take_ref, norm_ref, out_ref, sums, rows):
    n_x = keep_ref.shape[0]
    n = out_ref.shape[0] // n_x
    count = n * cap
    lines = n // GROUP
    step = n_x * TILE
    last = keep_ref[0, count:].astype(F32) + take_ref[0, count:].astype(F32)
    hi, lo = split2(last[:lines] + last[lines:])
    norm_hi, norm_lo = split2(norm_ref[:1])
    norm = jnp.where(iota((1, LANES), 1) < LANES // 2, norm_hi, norm_lo)
    extra = [
        jnp.concatenate([jnp.broadcast_to(v[g : g + 1], (GROUP, LANES)) for g in range(lines)], axis=0)
        for v in (hi, lo)
    ]
    extra.insert(1, jnp.broadcast_to(norm, (n, LANES)))
    for x in range(n_x):
        sums[x] = keep_ref[x, :count].astype(F32) + take_ref[x, :count].astype(F32)
        for r in range(cap):
            rows[pl.ds(x * TILE + r, n, stride=step), :] = sums[x, pl.ds(r, n, stride=cap), :]
        for r, v in enumerate(extra):
            rows[pl.ds(x * TILE + cap + r, n, stride=step), :] = v
    out_ref[...] = rows[...].astype(BF).reshape(out_ref.shape)


def back_rows(keep, take, norms, n, cap):
    n_x = keep.shape[0]
    return pl.pallas_call(
        functools.partial(back_kernel, cap),
        in_specs=in_vmem(3),
        out_specs=pl.BlockSpec(memory_space=pltpu.VMEM),
        out_shape=jax.ShapeDtypeStruct((n * n_x, TILE, LANES), BF),
        scratch_shapes=[
            pltpu.VMEM((n_x, n * cap, LANES), F32),
            pltpu.VMEM((n * n_x * TILE, LANES), F32),
        ],
        compiler_params=params(24),
        name="back_rows",
    )(keep, take, norms)


def grads_kernel(core_s, delta_ref, own_ref, other_ref, gate_ref, up_ref, down_ref, norm_ref):
    core = core_s[0]
    step = 2 * LANES
    for k, (out, which) in enumerate(((gate_ref, 0), (up_ref, 0), (down_ref, 1))):
        total = 0.0
        delta = delta_ref[k].astype(F32).T.astype(BF)
        for side, ref in ((core, own_ref), (1 - core, other_ref)):
            for s in range(0, HALF, step):
                g = dot(delta, ref[which, :, s : s + step])
                cols = pl.ds(pl.multiple_of(side * HALF + s, step), step)
                out[0, :, cols] = g.astype(BF)
                sq = g * g
                total = total + sq[:, :LANES] + sq[:, LANES:]
        norm_ref[k] = jnp.sum(total.T, axis=0, keepdims=True)


def grads(core, delta, own, other):
    feats = delta.shape[2]
    out = jax.ShapeDtypeStruct((1, feats, 2 * HALF), BF)
    return pl.pallas_call(
        grads_kernel,
        in_specs=in_smem(1) + in_vmem(3),
        out_specs=in_vmem(4),
        out_shape=[out, out, out, jax.ShapeDtypeStruct((3, 1, feats), F32)],
        compiler_params=params(24),
        name="grads",
    )(core, delta, own, other)


def end_kernel(cap, n_x, at_s, me_s, recv_ref, ids_ref, rank_ref, w_ref, tok_ref, route_ref, norm_ref):
    n = recv_ref.shape[0] // n_x
    count = ids_ref.shape[1]
    parts = recv_ref[...].reshape(n, n_x, TILE, LANES)
    norm_row = iota((n, TILE, LANES), 1) == cap + 1
    total = jnp.zeros((n, TILE, LANES), F32)
    for x in range(n_x):
        part = parts[:, x].astype(F32)
        total = total + jnp.where(norm_row & (at_s[0] // 2 != x), 0.0, part)
    hi, lo = split2(total.reshape(n * TILE, LANES))
    rows = jnp.concatenate([hi, lo], axis=0).astype(BF)
    o = iota((2 * n * TILE, count), 0) % (n * TILE)
    first = [ids_ref[k : k + 1, :] * TILE for k in range(2)]
    rank = [rank_ref[k : k + 1, :] for k in range(2)]
    pick = ones_at((o == first[0] + rank[0]) | (o == first[1] + rank[1]))
    tok_ref[...] = dot(pick, rows, 0, 0).astype(BF)
    route = []
    for k in range(2):
        pick = ones_at((o == first[k] + cap) | (o == first[k] + cap + 2))
        got = dot(rows, pick, 0, 0)
        use = iota((LANES, count), 0) == (me_s[0] % GROUP) * TILE + rank[k]
        route.append(jnp.sum(jnp.where(use, got, 0.0), axis=0, keepdims=True))
    route_ref[...] = jnp.concatenate(route, axis=0) / w_ref[...]
    sums = dot(ones_at(iota((TILE, 2 * n * TILE), 1) % TILE == cap + 1), rows)
    norm_ref[...] = sums[:1, : LANES // 2] + sums[:1, LANES // 2 :]


def end(at, me, recv, ids_t, rank, w_t, cap, n_x):
    count = ids_t.shape[1]
    return pl.pallas_call(
        functools.partial(end_kernel, cap, n_x),
        in_specs=in_smem(2) + in_vmem(4),
        out_specs=in_vmem(3),
        out_shape=[
            jax.ShapeDtypeStruct((count, LANES), BF),
            jax.ShapeDtypeStruct((2, count), F32),
            jax.ShapeDtypeStruct((1, LANES // 2), F32),
        ],
        compiler_params=params(16),
        name="end",
    )(at, me, recv, ids_t, rank, w_t)


def swap(v):
    return lax.ppermute(v, "c", [(0, 1), (1, 0)])


def local(tokens, out_grad, expert_ids, route_weights, gate_proj, up_proj, down_proj, shared_act):
    n = lax.axis_size(EP)
    cap = 5 * tokens.shape[0] * expert_ids.shape[1] // (4 * n)
    core = lax.axis_index("c").reshape(1)
    at = lax.axis_index(TP).reshape(1)
    me = lax.axis_index(EP).reshape(1)
    ids_t, w_t = expert_ids.T, route_weights.T
    here = (tokens, out_grad, shared_act, ids_t, w_t)
    here = [pltpu.with_memory_space_constraint(v, pltpu.HBM) for v in here]
    sent, rank = send_rows(at, me, *here, cap, n)
    recv = lax.all_to_all(sent, EP, 0, 0, tiled=True)
    own = unpack(recv, cap)
    other = swap(own)
    half = half_products(core, own, gate_proj, up_proj, down_proj)
    shared, norms = shared_sum(recv, cap)
    give, delta, inner = forward(core, half, other, gate_proj, up_proj, down_proj, cap)
    take = swap(give)
    keep = keep_shares(core, delta, inner, gate_proj, up_proj)
    back = back_rows(keep, take, norms, n, cap)
    returned = lax.all_to_all(back, (*EP, "x"), 0, 0, tiled=True)
    gate_grad, up_grad, down_grad, row_norms = grads(core, delta, own, other)
    token_grad, route_grad, shared_norms = end(
        at, me, returned, ids_t, rank, w_t, cap, lax.axis_size("x")
    )
    return (
        token_grad,
        route_grad.T,
        gate_grad,
        up_grad,
        down_grad,
        row_norms.transpose(1, 0, 2),
        shared.T,
        shared_norms.reshape(-1),
    )


def solution(mesh):
    torus = Mesh(mesh.devices.reshape(8, 8, mesh.shape["tp"] // 2, 2), (*EP, *TP))
    return jax.shard_map(
        local,
        mesh=torus,
        in_specs=(
            P(EP, None),
            P(EP, None),
            P(EP, None),
            P(EP, None),
            P(EP, TP, None),
            P(EP, TP, None),
            P(EP, TP, None),
            P(EP, None),
        ),
        out_specs=(
            P(EP, TP),
            P(EP, None),
            P(EP, TP, None),
            P(EP, TP, None),
            P(EP, TP, None),
            P(EP, None, TP),
            P(TP, EP),
            P(TP),
        ),
        check_vma=False,
    )
```

```python
import functools

import jax
import jax.numpy as jnp
from jax import lax
from jax.experimental import pallas as pl
from jax.experimental.pallas import tpu as pltpu
from jax.sharding import Mesh
from jax.sharding import PartitionSpec as P

EP = ("z", "y")
TP = ("x", "c")
BF, F32, I32 = jnp.bfloat16, jnp.float32, jnp.int32
LANES = 128
TILE = 8
HALF = TILE * LANES
SHARED = 2
GROUP = 16


def params(mib):
    return pltpu.CompilerParams(vmem_limit_bytes=mib * 1024 * 1024)


def in_vmem(n):
    return [pl.BlockSpec(memory_space=pltpu.VMEM)] * n


def in_smem(n):
    return [pl.BlockSpec(memory_space=pltpu.SMEM)] * n


def iota(shape, dim):
    return lax.broadcasted_iota(I32, shape, dim)


def ones_at(mask):
    return mask.astype(F32).astype(BF)


def dot(a, b, ca=1, cb=0):
    return lax.dot_general(a, b, (((ca,), (cb,)), ((), ())), preferred_element_type=F32)


def split2(v):
    hi = v.astype(BF).astype(F32)
    return hi, v - hi


def spread(ref, x):
    for j in range(TILE):
        cols = x[:, j * LANES : (j + 1) * LANES].astype(F32)
        ref[pl.ds(j, x.shape[0], stride=TILE), :] = cols


def gather_cols(ref, count, j):
    return ref[pl.ds(j, count, stride=TILE), :]


def send_kernel(
    cap, at_s, me_s, tok_ref, grad_ref, act_ref, ids_ref, w_ref, out_ref, rank_s,
    tok_v, grad_v, act_v, ids_s, w_s, seen_s, tok_t, grad_t, sems,
):
    del me_s
    count, width = grad_ref.shape
    experts = out_ref.shape[0]
    mine = pl.ds(pl.multiple_of((at_s[0] % 2) * HALF, HALF), HALF)
    line = pl.ds(pl.multiple_of((at_s[0] // 2) * LANES, LANES), LANES)
    pairs = (
        (act_ref.at[:, line], act_v),
        (grad_ref, grad_v),
        (tok_ref.at[:, mine], tok_v),
        (ids_ref, ids_s),
        (w_ref, w_s),
    )
    copies = [pltpu.make_async_copy(a, b, sems.at[i]) for i, (a, b) in enumerate(pairs)]
    for c in copies:
        c.start()
    for e in range(experts):
        seen_s[e] = 0
    out_ref[:, : 2 * cap] = jnp.zeros((experts, 2 * cap, TILE, LANES), BF)
    for c in copies:
        c.wait()
    spread(tok_t, tok_v[...])
    spread(grad_t, grad_v[:, mine])

    def one_token(t, carry):
        rows = pl.ds(pl.multiple_of(t * TILE, TILE), TILE)
        tok = tok_t[rows, :].astype(BF)
        grad = grad_t[rows, :]
        for k in range(2):
            e = ids_s[k, t]
            r = seen_s[e]
            seen_s[e] = r + 1
            rank_s[k, t] = r
            out_ref[e, r] = tok
            out_ref[e, cap + r] = (w_s[k, t] * grad).astype(BF)
        return carry

    lax.fori_loop(0, count, one_token, 0, unroll=8)

    half = LANES // 2
    act = act_v[...]
    swapped = jnp.concatenate([act[:, half:], act[:, :half]], axis=1)
    own = (at_s[0] % 2) * half
    keep = (iota(act.shape, 1) // half) * half == own
    twice = jnp.where(keep, act.astype(F32), swapped.astype(F32)).astype(BF)
    step = 2 * LANES
    block = width // experts
    for s in range(0, width, step):
        term = dot(grad_v[:, s : s + step], twice, 0, 0)
        term = term.reshape(step // block, 2, block // 2, LANES)
        lane = iota((step // block, block // 2, LANES), 2)
        both = jnp.where(lane < half, term[:, 0], term[:, 1]).astype(BF)
        out_ref[s // block : (s + step) // block, 2 * cap :] = both.reshape(
            step // block, SHARED, TILE, LANES
        )


def send_rows(at, me, tokens, out_grad, act, ids_t, w_t, cap, experts):
    count, width = out_grad.shape
    return pl.pallas_call(
        functools.partial(send_kernel, cap),
        in_specs=in_smem(2) + [pl.BlockSpec(memory_space=pltpu.HBM)] * 5,
        out_specs=in_vmem(1) + in_smem(1),
        out_shape=[
            jax.ShapeDtypeStruct((experts, 2 * cap + SHARED, TILE, LANES), BF),
            jax.ShapeDtypeStruct((2, count), I32),
        ],
        scratch_shapes=[
            pltpu.VMEM((count, HALF), BF),
            pltpu.VMEM((count, width), BF),
            pltpu.VMEM((count, LANES), BF),
            pltpu.SMEM((2, count), I32),
            pltpu.SMEM((2, count), F32),
            pltpu.SMEM((experts,), I32),
            pltpu.VMEM((count * TILE, LANES), F32),
            pltpu.VMEM((count * TILE, LANES), F32),
            pltpu.SemaphoreType.DMA((5,)),
        ],
        compiler_params=params(16),
        name="send_rows",
    )(at, me, tokens, out_grad, act, ids_t, w_t)


def shared_kernel(cap, recv_ref, out_ref, norm_ref):
    total = jnp.sum(recv_ref[:, 2 * cap :].astype(F32), axis=0).reshape(SHARED * TILE, LANES)
    half = LANES // 2
    out_ref[...] = jnp.concatenate([total[:, :half], total[:, half:]], axis=0)
    sq = jnp.sum(total * total, axis=0, keepdims=True)
    sq = sq + jnp.concatenate([sq[:, half:], sq[:, :half]], axis=1)
    norm_ref[...] = jnp.broadcast_to(sq, norm_ref.shape)


def shared_sum(recv, cap):
    return pl.pallas_call(
        functools.partial(shared_kernel, cap),
        in_specs=in_vmem(1),
        out_specs=in_vmem(2),
        out_shape=[
            jax.ShapeDtypeStruct((32, LANES // 2), F32),
            jax.ShapeDtypeStruct((TILE, LANES), F32),
        ],
        compiler_params=params(16),
        name="shared_sum",
    )(recv)


def unpack_kernel(cap, recv_ref, rows_ref, in_t, cot_t):
    n = recv_ref.shape[0]
    count = n * cap
    for k, ref in enumerate((in_t, cot_t)):
        tiles = recv_ref[:, k * cap : (k + 1) * cap].astype(F32)
        ref[...] = tiles.reshape(count * TILE, LANES)
        for j in range(TILE):
            cols = slice(j * LANES, (j + 1) * LANES)
            rows_ref[k, :, cols] = gather_cols(ref, count, j).astype(BF)


def unpack(recv, cap):
    count = recv.shape[0] * cap
    return pl.pallas_call(
        functools.partial(unpack_kernel, cap),
        in_specs=in_vmem(1),
        out_specs=pl.BlockSpec(memory_space=pltpu.VMEM),
        out_shape=jax.ShapeDtypeStruct((2, count, HALF), BF),
        scratch_shapes=[pltpu.VMEM((count * TILE, LANES), F32)] * 2,
        compiler_params=params(16),
        name="unpack",
    )(recv)


def products(side, rows_ref, gate_ref, up_ref, down_ref, sums):
    step = 2 * LANES
    for s in range(0, HALF, step):
        cols = pl.ds(pl.multiple_of(side * HALF + s, step), step)
        a, b = rows_ref[0, :, s : s + step], rows_ref[1, :, s : s + step]
        for k, (x, w) in enumerate(((a, gate_ref), (a, up_ref), (b, down_ref))):
            sums[k] = sums[k] + dot(x, w[0, :, cols], 1, 1)
    return sums


def half_kernel(core_s, own_ref, gate_ref, up_ref, down_ref, out_ref):
    sums = products(core_s[0], own_ref, gate_ref, up_ref, down_ref, [0.0] * 3)
    for k in range(3):
        out_ref[k] = sums[k]


def half_products(core, own, gate, up, down):
    return pl.pallas_call(
        half_kernel,
        in_specs=in_smem(1) + in_vmem(4),
        out_specs=pl.BlockSpec(memory_space=pltpu.VMEM),
        out_shape=jax.ShapeDtypeStruct((3, own.shape[1], gate.shape[1]), F32),
        compiler_params=params(16),
        name="half_products",
    )(core, own, gate, up, down)


def shares(side, deltas, gate_ref, up_ref, inner, ref):
    count = deltas.shape[0]
    for j in range(ref.shape[0]):
        cols = pl.ds(pl.multiple_of(j * 2 * LANES + side * LANES, LANES), LANES)
        w = jnp.concatenate([gate_ref[0, :, cols], up_ref[0, :, cols]], axis=0)
        ref[j, :count] = dot(deltas, w).astype(BF)
        ref[j, count:] = inner


def forward_kernel(
    cap, core_s, half_ref, other_ref, gate_ref, up_ref, down_ref, give_ref, delta_ref, inner_ref
):
    core = core_s[0]
    count = other_ref.shape[1]
    sums = products(1 - core, other_ref, gate_ref, up_ref, down_ref, [half_ref[k] for k in range(3)])
    gate_pre, up_pre, hidden_grad = sums
    sig = jax.nn.sigmoid(gate_pre)
    silu = gate_pre * sig
    hidden = (silu * up_pre).astype(BF)
    up_delta = (hidden_grad * silu).astype(BF)
    gate_delta = (hidden_grad * up_pre * sig * (1.0 + gate_pre * (1.0 - sig))).astype(BF)
    inner = jnp.sum(hidden.astype(F32) * hidden_grad, axis=1, keepdims=True)
    slot = iota((count, LANES), 0)
    lane = (slot // cap) % GROUP * TILE + slot % cap
    spots = jnp.where(lane == iota((count, LANES), 1), inner, 0.0)
    span = GROUP * cap
    lines = [jnp.sum(spots[s : s + span], axis=0, keepdims=True) for s in range(0, count, span)]
    tile = jnp.concatenate(split2(jnp.concatenate(lines, axis=0)), axis=0).astype(BF)
    inner_ref[...] = tile
    shares(1 - core, jnp.concatenate([gate_delta, up_delta], axis=1), gate_ref, up_ref, tile, give_ref)
    for k, d in enumerate((gate_delta, up_delta, hidden)):
        delta_ref[k] = d


def forward(core, half, other, gate, up, down, cap):
    count = other.shape[1]
    return pl.pallas_call(
        functools.partial(forward_kernel, cap),
        in_specs=in_smem(1) + in_vmem(5),
        out_specs=in_vmem(3),
        out_shape=[
            jax.ShapeDtypeStruct((TILE, count + TILE, LANES), BF),
            jax.ShapeDtypeStruct((3, count, gate.shape[1]), BF),
            jax.ShapeDtypeStruct((TILE, LANES), BF),
        ],
        compiler_params=params(24),
        name="forward",
    )(core, half, other, gate, up, down)


def keep_kernel(core_s, delta_ref, inner_ref, gate_ref, up_ref, keep_ref):
    deltas = jnp.concatenate([delta_ref[0], delta_ref[1]], axis=1)
    shares(core_s[0], deltas, gate_ref, up_ref, inner_ref[...], keep_ref)


def keep_shares(core, delta, inner, gate, up):
    return pl.pallas_call(
        keep_kernel,
        in_specs=in_smem(1) + in_vmem(4),
        out_specs=pl.BlockSpec(memory_space=pltpu.VMEM),
        out_shape=jax.ShapeDtypeStruct((TILE, delta.shape[1] + TILE, LANES), BF),
        compiler_params=params(16),
        name="keep_shares",
    )(core, delta, inner, gate, up)


def pair_kernel(a_ref, b_ref, out_ref):
    out_ref[...] = (a_ref[...].astype(F32) + b_ref[...].astype(F32)).astype(BF)


def pair_sum(a, b):
    return pl.pallas_call(
        pair_kernel,
        in_specs=in_vmem(2),
        out_specs=pl.BlockSpec(memory_space=pltpu.VMEM),
        out_shape=jax.ShapeDtypeStruct(a.shape, BF),
        compiler_params=params(16),
        name="pair_sum",
    )(a, b)


def grads_kernel(core_s, delta_ref, own_ref, other_ref, gate_ref, up_ref, down_ref, norm_ref):
    core = core_s[0]
    step = 2 * LANES
    for k, (out, which) in enumerate(((gate_ref, 0), (up_ref, 0), (down_ref, 1))):
        total = 0.0
        delta = delta_ref[k].astype(F32).T.astype(BF)
        for side, ref in ((core, own_ref), (1 - core, other_ref)):
            for s in range(0, HALF, step):
                g = dot(delta, ref[which, :, s : s + step])
                cols = pl.ds(pl.multiple_of(side * HALF + s, step), step)
                out[0, :, cols] = g.astype(BF)
                sq = g * g
                total = total + sq[:, :LANES] + sq[:, LANES:]
        norm_ref[k] = jnp.sum(total.T, axis=0, keepdims=True)


def grads(core, delta, own, other):
    feats = delta.shape[2]
    out = jax.ShapeDtypeStruct((1, feats, 2 * HALF), BF)
    return pl.pallas_call(
        grads_kernel,
        in_specs=in_smem(1) + in_vmem(3),
        out_specs=in_vmem(4),
        out_shape=[out, out, out, jax.ShapeDtypeStruct((3, 1, feats), F32)],
        compiler_params=params(24),
        name="grads",
    )(core, delta, own, other)


def back_kernel(cap, parts_ref, norm_ref, out_ref, sums, rows):
    n = out_ref.shape[0]
    count = n * cap
    total = parts_ref[0].astype(F32)
    for x in range(1, parts_ref.shape[0]):
        total = total + parts_ref[x].astype(F32)
    sums[...] = total
    for r in range(cap):
        rows[pl.ds(r, n, stride=TILE), :] = sums[pl.ds(r, n, stride=cap), :]
    lines = n // GROUP
    inner = split2(total[count : count + lines] + total[count + lines : count + 2 * lines])
    for r, part in zip((cap, cap + 2), inner):
        spread_lines = [
            jnp.broadcast_to(part[g : g + 1], (GROUP, LANES)) for g in range(lines)
        ]
        rows[pl.ds(r, n, stride=TILE), :] = jnp.concatenate(spread_lines, axis=0)
    norm_hi, norm_lo = split2(norm_ref[:1])
    norm = jnp.where(iota((1, LANES), 1) < LANES // 2, norm_hi, norm_lo)
    rows[pl.ds(cap + 1, n, stride=TILE), :] = jnp.broadcast_to(norm, (n, LANES))
    out_ref[...] = rows[...].astype(BF).reshape(n, TILE, LANES)


def back_rows(parts, norms, n, cap):
    return pl.pallas_call(
        functools.partial(back_kernel, cap),
        in_specs=in_vmem(2),
        out_specs=pl.BlockSpec(memory_space=pltpu.VMEM),
        out_shape=jax.ShapeDtypeStruct((n, TILE, LANES), BF),
        scratch_shapes=[
            pltpu.VMEM(parts.shape[1:], F32),
            pltpu.VMEM((n * TILE, LANES), F32),
        ],
        compiler_params=params(16),
        name="back_rows",
    )(parts, norms)


def end_kernel(cap, me_s, recv_ref, ids_ref, rank_ref, w_ref, tok_ref, route_ref, norm_ref):
    n = recv_ref.shape[0]
    count = ids_ref.shape[1]
    rows = recv_ref[...].reshape(n * TILE, LANES)
    o = iota((n * TILE, count), 0)
    first = [ids_ref[k : k + 1, :] * TILE for k in range(2)]
    rank = [rank_ref[k : k + 1, :] for k in range(2)]
    pick = ones_at((o == first[0] + rank[0]) | (o == first[1] + rank[1]))
    tok_ref[...] = dot(pick, rows, 0, 0).astype(BF)
    route = []
    for k in range(2):
        pick = ones_at((o == first[k] + cap) | (o == first[k] + cap + 2))
        got = dot(rows, pick, 0, 0)
        use = iota((LANES, count), 0) == (me_s[0] % GROUP) * TILE + rank[k]
        route.append(jnp.sum(jnp.where(use, got, 0.0), axis=0, keepdims=True))
    route_ref[...] = jnp.concatenate(route, axis=0) / w_ref[...]
    sums = dot(ones_at(iota((TILE, n * TILE), 1) % TILE == cap + 1), rows)
    norm_ref[...] = sums[:1, : LANES // 2] + sums[:1, LANES // 2 :]


def end(me, recv, ids_t, rank, w_t, cap):
    count = ids_t.shape[1]
    return pl.pallas_call(
        functools.partial(end_kernel, cap),
        in_specs=in_smem(1) + in_vmem(4),
        out_specs=in_vmem(3),
        out_shape=[
            jax.ShapeDtypeStruct((count, LANES), BF),
            jax.ShapeDtypeStruct((2, count), F32),
            jax.ShapeDtypeStruct((1, LANES // 2), F32),
        ],
        compiler_params=params(16),
        name="end",
    )(me, recv, ids_t, rank, w_t)


def swap(v):
    return lax.ppermute(v, "c", [(0, 1), (1, 0)])


def local(tokens, out_grad, expert_ids, route_weights, gate_proj, up_proj, down_proj, shared_act):
    n = lax.axis_size(EP)
    cap = 5 * tokens.shape[0] * expert_ids.shape[1] // (4 * n)
    core = lax.axis_index("c").reshape(1)
    at = lax.axis_index(TP).reshape(1)
    me = lax.axis_index(EP).reshape(1)
    ids_t, w_t = expert_ids.T, route_weights.T
    here = (tokens, out_grad, shared_act, ids_t, w_t)
    here = [pltpu.with_memory_space_constraint(v, pltpu.HBM) for v in here]
    sent, rank = send_rows(at, me, *here, cap, n)
    recv = lax.all_to_all(sent, EP, 0, 0, tiled=True)
    own = unpack(recv, cap)
    other = swap(own)
    half = half_products(core, own, gate_proj, up_proj, down_proj)
    shared, norms = shared_sum(recv, cap)
    give, delta, inner = forward(core, half, other, gate_proj, up_proj, down_proj, cap)
    take = swap(give)
    keep = keep_shares(core, delta, inner, gate_proj, up_proj)
    summed, norms = lax.optimization_barrier((pair_sum(keep, take), norms))
    parts = lax.all_to_all(summed, "x", 0, 0, tiled=True)
    back = back_rows(parts, norms, n, cap)
    back, delta = lax.optimization_barrier((back, delta))
    gate_grad, up_grad, down_grad, row_norms = grads(core, delta, own, other)
    returned = lax.all_to_all(back, EP, 0, 0, tiled=True)
    token_grad, route_grad, shared_norms = end(me, returned, ids_t, rank, w_t, cap)
    return (
        token_grad,
        route_grad.T,
        gate_grad,
        up_grad,
        down_grad,
        row_norms.transpose(1, 0, 2),
        shared.T,
        shared_norms.reshape(-1),
    )


def solution(mesh):
    torus = Mesh(mesh.devices.reshape(8, 8, mesh.shape["tp"] // 2, 2), (*EP, *TP))
    return jax.shard_map(
        local,
        mesh=torus,
        in_specs=(
            P(EP, None),
            P(EP, None),
            P(EP, None),
            P(EP, None),
            P(EP, TP, None),
            P(EP, TP, None),
            P(EP, TP, None),
            P(EP, None),
        ),
        out_specs=(
            P(EP, TP),
            P(EP, None),
            P(EP, TP, None),
            P(EP, TP, None),
            P(EP, TP, None),
            P(EP, None, TP),
            P(TP, EP),
            P(TP),
        ),
        check_vma=False,
    )
```

```python
import functools

import jax
import jax.numpy as jnp
from jax import lax
from jax.experimental import pallas as pl
from jax.experimental.pallas import tpu as pltpu
from jax.sharding import Mesh
from jax.sharding import PartitionSpec as P

EP = ("z", "y")
TP = ("x", "c")
BF, F32, I32 = jnp.bfloat16, jnp.float32, jnp.int32
LANES = 128
TILE = 8
HALF = TILE * LANES
SHARED = 2
GROUP = 16


def params(mib):
    return pltpu.CompilerParams(vmem_limit_bytes=mib * 1024 * 1024)


def in_vmem(n):
    return [pl.BlockSpec(memory_space=pltpu.VMEM)] * n


def in_smem(n):
    return [pl.BlockSpec(memory_space=pltpu.SMEM)] * n


def iota(shape, dim):
    return lax.broadcasted_iota(I32, shape, dim)


def ones_at(mask):
    return mask.astype(F32).astype(BF)


def dot(a, b, ca=1, cb=0):
    return lax.dot_general(a, b, (((ca,), (cb,)), ((), ())), preferred_element_type=F32)


def split2(v):
    hi = v.astype(BF).astype(F32)
    return hi, v - hi


def spread(ref, x):
    for j in range(TILE):
        cols = x[:, j * LANES : (j + 1) * LANES].astype(F32)
        ref[pl.ds(j, x.shape[0], stride=TILE), :] = cols


def gather_cols(ref, count, j):
    return ref[pl.ds(j, count, stride=TILE), :]


def send_kernel(
    cap, at_s, me_s, tok_ref, grad_ref, act_ref, ids_ref, w_ref, out_ref, rank_s,
    tok_v, grad_v, act_v, ids_s, w_s, seen_s, tok_t, grad_t, sems,
):
    del me_s
    count, width = grad_ref.shape
    experts = out_ref.shape[0]
    mine = pl.ds(pl.multiple_of((at_s[0] % 2) * HALF, HALF), HALF)
    line = pl.ds(pl.multiple_of((at_s[0] // 2) * LANES, LANES), LANES)
    pairs = (
        (act_ref.at[:, line], act_v),
        (grad_ref, grad_v),
        (tok_ref.at[:, mine], tok_v),
        (ids_ref, ids_s),
        (w_ref, w_s),
    )
    copies = [pltpu.make_async_copy(a, b, sems.at[i]) for i, (a, b) in enumerate(pairs)]
    for c in copies:
        c.start()
    for e in range(experts):
        seen_s[e] = 0
    out_ref[:, : 2 * cap] = jnp.zeros((experts, 2 * cap, TILE, LANES), BF)
    for c in copies:
        c.wait()
    spread(tok_t, tok_v[...])
    spread(grad_t, grad_v[:, mine])

    half = LANES // 2
    act = act_v[...]
    swapped = jnp.concatenate([act[:, half:], act[:, :half]], axis=1)
    own = (at_s[0] % 2) * half
    keep = (iota(act.shape, 1) // half) * half == own
    twice = jnp.where(keep, act.astype(F32), swapped.astype(F32)).astype(BF)
    step = 2 * LANES
    block = width // experts
    n = step // block
    steps = width // step

    def one_step(i, carry):
        for j in range(count // steps):
            t = i * (count // steps) + j
            rows = pl.ds(pl.multiple_of(t * TILE, TILE), TILE)
            tok = tok_t[rows, :].astype(BF)
            grad = grad_t[rows, :]
            for k in range(2):
                e = ids_s[k, t]
                r = seen_s[e]
                seen_s[e] = r + 1
                rank_s[k, t] = r
                out_ref[e, r] = tok
                out_ref[e, cap + r] = (w_s[k, t] * grad).astype(BF)
        cols = pl.ds(pl.multiple_of(i * step, step), step)
        term = dot(grad_v[:, cols], twice, 0, 0).reshape(n, 2, block // 2, LANES)
        left = iota((n, block // 2, LANES), 2) < half
        both = jnp.where(left, term[:, 0], term[:, 1]).astype(BF)
        out_ref[pl.ds(i * n, n), 2 * cap :] = both.reshape(n, SHARED, TILE, LANES)
        return carry

    lax.fori_loop(0, steps, one_step, 0)


def send_rows(at, me, tokens, out_grad, act, ids_t, w_t, cap, experts):
    count, width = out_grad.shape
    return pl.pallas_call(
        functools.partial(send_kernel, cap),
        in_specs=in_smem(2) + [pl.BlockSpec(memory_space=pltpu.HBM)] * 5,
        out_specs=in_vmem(1) + in_smem(1),
        out_shape=[
            jax.ShapeDtypeStruct((experts, 2 * cap + SHARED, TILE, LANES), BF),
            jax.ShapeDtypeStruct((2, count), I32),
        ],
        scratch_shapes=[
            pltpu.VMEM((count, HALF), BF),
            pltpu.VMEM((count, width), BF),
            pltpu.VMEM((count, LANES), BF),
            pltpu.SMEM((2, count), I32),
            pltpu.SMEM((2, count), F32),
            pltpu.SMEM((experts,), I32),
            pltpu.VMEM((count * TILE, LANES), F32),
            pltpu.VMEM((count * TILE, LANES), F32),
            pltpu.SemaphoreType.DMA((5,)),
        ],
        compiler_params=params(16),
        name="send_rows",
    )(at, me, tokens, out_grad, act, ids_t, w_t)


def shared_kernel(cap, recv_ref, out_ref, norm_ref):
    total = jnp.sum(recv_ref[:, 2 * cap :].astype(F32), axis=0).reshape(SHARED * TILE, LANES)
    half = LANES // 2
    out_ref[...] = jnp.concatenate([total[:, :half], total[:, half:]], axis=0)
    sq = jnp.sum(total * total, axis=0, keepdims=True)
    sq = sq + jnp.concatenate([sq[:, half:], sq[:, :half]], axis=1)
    norm_ref[...] = jnp.broadcast_to(sq, norm_ref.shape)


def shared_sum(recv, cap):
    return pl.pallas_call(
        functools.partial(shared_kernel, cap),
        in_specs=in_vmem(1),
        out_specs=in_vmem(2),
        out_shape=[
            jax.ShapeDtypeStruct((32, LANES // 2), F32),
            jax.ShapeDtypeStruct((TILE, LANES), F32),
        ],
        compiler_params=params(16),
        name="shared_sum",
    )(recv)


def unpack_kernel(cap, recv_ref, rows_ref, in_t, cot_t):
    n = recv_ref.shape[0]
    count = n * cap
    for k, ref in enumerate((in_t, cot_t)):
        tiles = recv_ref[:, k * cap : (k + 1) * cap].astype(F32)
        ref[...] = tiles.reshape(count * TILE, LANES)
        for j in range(TILE):
            cols = slice(j * LANES, (j + 1) * LANES)
            rows_ref[k, :, cols] = gather_cols(ref, count, j).astype(BF)


def unpack(recv, cap):
    count = recv.shape[0] * cap
    return pl.pallas_call(
        functools.partial(unpack_kernel, cap),
        in_specs=in_vmem(1),
        out_specs=pl.BlockSpec(memory_space=pltpu.VMEM),
        out_shape=jax.ShapeDtypeStruct((2, count, HALF), BF),
        scratch_shapes=[pltpu.VMEM((count * TILE, LANES), F32)] * 2,
        compiler_params=params(16),
        name="unpack",
    )(recv)


def products(side, rows_ref, gate_ref, up_ref, down_ref, sums):
    step = 2 * LANES
    for s in range(0, HALF, step):
        cols = pl.ds(pl.multiple_of(side * HALF + s, step), step)
        a, b = rows_ref[0, :, s : s + step], rows_ref[1, :, s : s + step]
        for k, (x, w) in enumerate(((a, gate_ref), (a, up_ref), (b, down_ref))):
            sums[k] = sums[k] + dot(x, w[0, :, cols], 1, 1)
    return sums


def columns(ref, x, side):
    return ref[0, :, pl.ds(pl.multiple_of((2 * x + side) * LANES, LANES), LANES)]


def half_kernel(core_s, own_ref, gate_ref, up_ref, down_ref, out_ref, give_ref):
    for x in range(give_ref.shape[1] // LANES):
        pair = [columns(ref, x, 1 - core_s[0]) for ref in (gate_ref, up_ref)]
        give_ref[:, x * LANES : (x + 1) * LANES] = jnp.concatenate(pair, axis=0)
    sums = products(core_s[0], own_ref, gate_ref, up_ref, down_ref, [0.0] * 3)
    for k in range(3):
        out_ref[k] = sums[k]


def half_products(core, own, gate, up, down):
    feats = gate.shape[1]
    return pl.pallas_call(
        half_kernel,
        in_specs=in_smem(1) + in_vmem(4),
        out_specs=in_vmem(2),
        out_shape=[
            jax.ShapeDtypeStruct((3, own.shape[1], feats), F32),
            jax.ShapeDtypeStruct((2 * feats, HALF), BF),
        ],
        compiler_params=params(16),
        name="half_products",
    )(core, own, gate, up, down)


def forward_kernel(
    cap, core_s, half_ref, other_ref, gate_ref, up_ref, down_ref, give_ref, hidden_ref
):
    core = core_s[0]
    count = other_ref.shape[1]
    sums = products(1 - core, other_ref, gate_ref, up_ref, down_ref, [half_ref[k] for k in range(3)])
    gate_pre, up_pre, hidden_grad = sums
    sig = jax.nn.sigmoid(gate_pre)
    silu = gate_pre * sig
    hidden = (silu * up_pre).astype(BF)
    hidden_ref[...] = hidden
    up_delta = (hidden_grad * silu).astype(BF)
    gate_delta = (hidden_grad * up_pre * sig * (1.0 + gate_pre * (1.0 - sig))).astype(BF)
    give_ref[:count] = gate_delta
    give_ref[count : 2 * count] = up_delta
    inner = jnp.sum(hidden.astype(F32) * hidden_grad, axis=1, keepdims=True)
    slot = iota((count, LANES), 0)
    lane = (slot // cap) % GROUP * TILE + slot % cap
    spots = jnp.where(lane == iota((count, LANES), 1), inner, 0.0)
    span = GROUP * cap
    lines = [jnp.sum(spots[s : s + span], axis=0, keepdims=True) for s in range(0, count, span)]
    tile = jnp.concatenate(split2(jnp.concatenate(lines, axis=0)), axis=0)
    give_ref[2 * count :] = tile.astype(BF)


def forward(core, half, other, gate, up, down, cap):
    count = other.shape[1]
    feats = gate.shape[1]
    return pl.pallas_call(
        functools.partial(forward_kernel, cap),
        in_specs=in_smem(1) + in_vmem(5),
        out_specs=in_vmem(2),
        out_shape=[
            jax.ShapeDtypeStruct((2 * count + TILE, feats), BF),
            jax.ShapeDtypeStruct((count, feats), BF),
        ],
        compiler_params=params(24),
        name="forward",
    )(core, half, other, gate, up, down)


def shares_kernel(core_s, give_ref, take_ref, cols_ref, gate_ref, up_ref, out_ref):
    count = (give_ref.shape[0] - TILE) // 2
    deltas = [ref[k * count : (k + 1) * count] for ref in (give_ref, take_ref) for k in range(2)]
    deltas = jnp.concatenate(deltas, axis=1)
    last = give_ref[2 * count :].astype(F32) + take_ref[2 * count :].astype(F32)
    inner = split2(last[: TILE // 2] + last[TILE // 2 :])
    inner = jnp.concatenate(inner, axis=0).astype(BF)
    for x in range(out_ref.shape[0]):
        pair = [columns(ref, x, core_s[0]) for ref in (gate_ref, up_ref)]
        pair.append(cols_ref[:, x * LANES : (x + 1) * LANES])
        out_ref[x, :count] = dot(deltas, jnp.concatenate(pair, axis=0)).astype(BF)
        out_ref[x, count:] = inner


def shares(core, give, take, cols, gate, up):
    count = (give.shape[0] - TILE) // 2
    return pl.pallas_call(
        shares_kernel,
        in_specs=in_smem(1) + in_vmem(5),
        out_specs=pl.BlockSpec(memory_space=pltpu.VMEM),
        out_shape=jax.ShapeDtypeStruct((TILE, count + TILE, LANES), BF),
        compiler_params=params(16),
        name="shares",
    )(core, give, take, cols, gate, up)


def grads_kernel(
    core_s, give_ref, hidden_ref, own_ref, other_ref, gate_ref, up_ref, down_ref, norm_ref
):
    core = core_s[0]
    count = hidden_ref.shape[0]
    deltas = (give_ref[:count], give_ref[count : 2 * count], hidden_ref[...])
    step = 2 * LANES
    for k, (out, which) in enumerate(((gate_ref, 0), (up_ref, 0), (down_ref, 1))):
        total = 0.0
        delta = deltas[k].astype(F32).T.astype(BF)
        for side, ref in ((core, own_ref), (1 - core, other_ref)):
            for s in range(0, HALF, step):
                g = dot(delta, ref[which, :, s : s + step])
                cols = pl.ds(pl.multiple_of(side * HALF + s, step), step)
                out[0, :, cols] = g.astype(BF)
                sq = g * g
                total = total + sq[:, :LANES] + sq[:, LANES:]
        norm_ref[k] = jnp.sum(total.T, axis=0, keepdims=True)


def grads(core, give, hidden, own, other):
    feats = hidden.shape[1]
    out = jax.ShapeDtypeStruct((1, feats, 2 * HALF), BF)
    return pl.pallas_call(
        grads_kernel,
        in_specs=in_smem(1) + in_vmem(4),
        out_specs=in_vmem(4),
        out_shape=[out, out, out, jax.ShapeDtypeStruct((3, 1, feats), F32)],
        compiler_params=params(24),
        name="grads",
    )(core, give, hidden, own, other)


def back_kernel(cap, parts_ref, norm_ref, out_ref, sums, rows):
    n = out_ref.shape[0]
    count = n * cap
    total = parts_ref[0].astype(F32)
    for x in range(1, parts_ref.shape[0]):
        total = total + parts_ref[x].astype(F32)
    sums[...] = total
    for r in range(cap):
        rows[pl.ds(r, n, stride=TILE), :] = sums[pl.ds(r, n, stride=cap), :]
    lines = n // GROUP
    inner = split2(total[count : count + lines] + total[count + lines : count + 2 * lines])
    for r, part in zip((cap, cap + 2), inner):
        spread_lines = [
            jnp.broadcast_to(part[g : g + 1], (GROUP, LANES)) for g in range(lines)
        ]
        rows[pl.ds(r, n, stride=TILE), :] = jnp.concatenate(spread_lines, axis=0)
    norm_hi, norm_lo = split2(norm_ref[:1])
    norm = jnp.where(iota((1, LANES), 1) < LANES // 2, norm_hi, norm_lo)
    rows[pl.ds(cap + 1, n, stride=TILE), :] = jnp.broadcast_to(norm, (n, LANES))
    out_ref[...] = rows[...].astype(BF).reshape(n, TILE, LANES)


def back_rows(parts, norms, n, cap):
    return pl.pallas_call(
        functools.partial(back_kernel, cap),
        in_specs=in_vmem(2),
        out_specs=pl.BlockSpec(memory_space=pltpu.VMEM),
        out_shape=jax.ShapeDtypeStruct((n, TILE, LANES), BF),
        scratch_shapes=[
            pltpu.VMEM(parts.shape[1:], F32),
            pltpu.VMEM((n * TILE, LANES), F32),
        ],
        compiler_params=params(16),
        name="back_rows",
    )(parts, norms)


def end_kernel(cap, me_s, recv_ref, ids_ref, rank_ref, w_ref, tok_ref, route_ref, norm_ref):
    n = recv_ref.shape[0]
    count = ids_ref.shape[1]
    rows = recv_ref[...].reshape(n * TILE, LANES)
    o = iota((n * TILE, count), 0)
    first = [ids_ref[k : k + 1, :] * TILE for k in range(2)]
    rank = [rank_ref[k : k + 1, :] for k in range(2)]
    pick = ones_at((o == first[0] + rank[0]) | (o == first[1] + rank[1]))
    tok_ref[...] = dot(pick, rows, 0, 0).astype(BF)
    route = []
    for k in range(2):
        pick = ones_at((o == first[k] + cap) | (o == first[k] + cap + 2))
        got = dot(rows, pick, 0, 0)
        use = iota((LANES, count), 0) == (me_s[0] % GROUP) * TILE + rank[k]
        route.append(jnp.sum(jnp.where(use, got, 0.0), axis=0, keepdims=True))
    route_ref[...] = jnp.concatenate(route, axis=0) / w_ref[...]
    sums = dot(ones_at(iota((TILE, n * TILE), 1) % TILE == cap + 1), rows)
    norm_ref[...] = sums[:1, : LANES // 2] + sums[:1, LANES // 2 :]


def end(me, recv, ids_t, rank, w_t, cap):
    count = ids_t.shape[1]
    return pl.pallas_call(
        functools.partial(end_kernel, cap),
        in_specs=in_smem(1) + in_vmem(4),
        out_specs=in_vmem(3),
        out_shape=[
            jax.ShapeDtypeStruct((count, LANES), BF),
            jax.ShapeDtypeStruct((2, count), F32),
            jax.ShapeDtypeStruct((1, LANES // 2), F32),
        ],
        compiler_params=params(16),
        name="end",
    )(me, recv, ids_t, rank, w_t)


def swap(v):
    return lax.ppermute(v, "c", [(0, 1), (1, 0)])


def local(tokens, out_grad, expert_ids, route_weights, gate_proj, up_proj, down_proj, shared_act):
    n = lax.axis_size(EP)
    cap = 5 * tokens.shape[0] * expert_ids.shape[1] // (4 * n)
    core = lax.axis_index("c").reshape(1)
    at = lax.axis_index(TP).reshape(1)
    me = lax.axis_index(EP).reshape(1)
    ids_t, w_t = expert_ids.T, route_weights.T
    here = (tokens, out_grad, shared_act, ids_t, w_t)
    here = [pltpu.with_memory_space_constraint(v, pltpu.HBM) for v in here]
    sent, rank = send_rows(at, me, *here, cap, n)
    recv = lax.all_to_all(sent, EP, 0, 0, tiled=True)
    own = unpack(recv, cap)
    other = swap(own)
    half, cols = half_products(core, own, gate_proj, up_proj, down_proj)
    cols = swap(cols)
    shared, norms = shared_sum(recv, cap)
    give, hidden = forward(core, half, other, gate_proj, up_proj, down_proj, cap)
    part = shares(core, give, swap(give), cols, gate_proj, up_proj)
    part, norms = lax.optimization_barrier((part, norms))
    back = back_rows(lax.all_to_all(part, "x", 0, 0, tiled=True), norms, n, cap)
    back, hidden = lax.optimization_barrier((back, hidden))
    gate_grad, up_grad, down_grad, row_norms = grads(core, give, hidden, own, other)
    returned = lax.all_to_all(back, EP, 0, 0, tiled=True)
    token_grad, route_grad, shared_norms = end(me, returned, ids_t, rank, w_t, cap)
    return (
        token_grad,
        route_grad.T,
        gate_grad,
        up_grad,
        down_grad,
        row_norms.transpose(1, 0, 2),
        shared.T,
        shared_norms.reshape(-1),
    )


def solution(mesh):
    torus = Mesh(mesh.devices.reshape(8, 8, mesh.shape["tp"] // 2, 2), (*EP, *TP))
    return jax.shard_map(
        local,
        mesh=torus,
        in_specs=(
            P(EP, None),
            P(EP, None),
            P(EP, None),
            P(EP, None),
            P(EP, TP, None),
            P(EP, TP, None),
            P(EP, TP, None),
            P(EP, None),
        ),
        out_specs=(
            P(EP, TP),
            P(EP, None),
            P(EP, TP, None),
            P(EP, TP, None),
            P(EP, TP, None),
            P(EP, None, TP),
            P(TP, EP),
            P(TP),
        ),
        check_vma=False,
    )
```

```python
import functools

import jax
import jax.numpy as jnp
from jax import lax
from jax.experimental import pallas as pl
from jax.experimental.pallas import tpu as pltpu
from jax.sharding import Mesh
from jax.sharding import PartitionSpec as P

EP = ("z", "y")
TP = ("x", "c")
BF, F32, I32 = jnp.bfloat16, jnp.float32, jnp.int32
LANES = 128
TILE = 8
HALF = TILE * LANES
SHARED = 2
GROUP = 16


def params(mib):
    return pltpu.CompilerParams(vmem_limit_bytes=mib * 1024 * 1024)


def in_vmem(n):
    return [pl.BlockSpec(memory_space=pltpu.VMEM)] * n


def in_smem(n):
    return [pl.BlockSpec(memory_space=pltpu.SMEM)] * n


def iota(shape, dim):
    return lax.broadcasted_iota(I32, shape, dim)


def ones_at(mask):
    return mask.astype(F32).astype(BF)


def dot(a, b, ca=1, cb=0):
    return lax.dot_general(a, b, (((ca,), (cb,)), ((), ())), preferred_element_type=F32)


def split2(v):
    hi = v.astype(BF).astype(F32)
    return hi, v - hi


def spread(ref, x):
    for j in range(TILE):
        cols = x[:, j * LANES : (j + 1) * LANES].astype(F32)
        ref[pl.ds(j, x.shape[0], stride=TILE), :] = cols


def gather_cols(ref, count, j):
    return ref[pl.ds(j, count, stride=TILE), :]


def send_kernel(
    cap, at_s, me_s, tok_ref, grad_ref, act_ref, ids_ref, w_ref, out_ref, slot_s,
    tok_v, grad_v, act_v, ids_s, w_s, next_s, tok_t, grad_t, sems,
):
    del me_s
    count, width = grad_ref.shape
    block = 2 * cap + SHARED
    experts = out_ref.shape[0] // block
    mine = pl.ds(pl.multiple_of((at_s[0] % 2) * HALF, HALF), HALF)
    line = pl.ds(pl.multiple_of((at_s[0] // 2) * LANES, LANES), LANES)
    pairs = (
        (grad_ref, grad_v),
        (tok_ref.at[:, mine], tok_v),
        (ids_ref, ids_s),
        (w_ref, w_s),
        (act_ref.at[:, line], act_v),
    )
    copies = [pltpu.make_async_copy(a, b, sems.at[i]) for i, (a, b) in enumerate(pairs)]
    for c in copies:
        c.start()

    def clear(e, carry):
        next_s[e] = e * block
        out_ref[pl.ds(e * block, 2 * cap)] = jnp.zeros((2 * cap, TILE, LANES), BF)
        return carry

    lax.fori_loop(0, experts, clear, 0, unroll=4)
    for c in copies:
        c.wait()
    spread(tok_t, tok_v[...])
    spread(grad_t, grad_v[:, mine])

    def one_token(t, carry):
        rows = pl.ds(pl.multiple_of(t * TILE, TILE), TILE)
        tok = tok_t[rows, :].astype(BF)
        grad = grad_t[rows, :]
        for k in range(2):
            e = ids_s[k, t]
            i = next_s[e]
            next_s[e] = i + 1
            slot_s[k, t] = i
            out_ref[i] = tok
            out_ref[i + cap] = (w_s[k, t] * grad).astype(BF)
        return carry

    lax.fori_loop(0, count, one_token, 0, unroll=8)

    half = LANES // 2
    act = act_v[...]
    swapped = jnp.concatenate([act[:, half:], act[:, :half]], axis=1)
    own = (at_s[0] % 2) * half
    keep = (iota(act.shape, 1) // half) * half == own
    twice = jnp.where(keep, act.astype(F32), swapped.astype(F32)).astype(BF)
    step = 2 * LANES
    cols = width // experts
    for s in range(0, width, step):
        term = dot(grad_v[:, s : s + step], twice, 0, 0)
        term = term.reshape(step // cols, 2, cols // 2, LANES)
        left = iota((step // cols, cols // 2, LANES), 2) < half
        both = jnp.where(left, term[:, 0], term[:, 1]).astype(BF)
        for e in range(step // cols):
            at = (s // cols + e) * block + 2 * cap
            out_ref[at : at + SHARED] = both[e].reshape(SHARED, TILE, LANES)


def send_rows(at, me, tokens, out_grad, act, ids_t, w_t, cap, experts):
    count, width = out_grad.shape
    block = 2 * cap + SHARED
    sent, slots = pl.pallas_call(
        functools.partial(send_kernel, cap),
        in_specs=in_smem(2) + [pl.BlockSpec(memory_space=pltpu.HBM)] * 5,
        out_specs=in_vmem(1) + in_smem(1),
        out_shape=[
            jax.ShapeDtypeStruct((experts * block, TILE, LANES), BF),
            jax.ShapeDtypeStruct((2, count), I32),
        ],
        scratch_shapes=[
            pltpu.VMEM((count, HALF), BF),
            pltpu.VMEM((count, width), BF),
            pltpu.VMEM((count, LANES), BF),
            pltpu.SMEM((2, count), I32),
            pltpu.SMEM((2, count), F32),
            pltpu.SMEM((experts,), I32),
            pltpu.VMEM((count * TILE, LANES), F32),
            pltpu.VMEM((count * TILE, LANES), F32),
            pltpu.SemaphoreType.DMA((5,)),
        ],
        compiler_params=params(16),
        name="send_rows",
    )(at, me, tokens, out_grad, act, ids_t, w_t)
    return sent.reshape(experts, block, TILE, LANES), slots


def shared_kernel(cap, recv_ref, out_ref, norm_ref):
    total = jnp.sum(recv_ref[:, 2 * cap :].astype(F32), axis=0).reshape(SHARED * TILE, LANES)
    half = LANES // 2
    out_ref[...] = jnp.concatenate([total[:, :half], total[:, half:]], axis=0)
    sq = jnp.sum(total * total, axis=0, keepdims=True)
    sq = sq + jnp.concatenate([sq[:, half:], sq[:, :half]], axis=1)
    norm_ref[...] = jnp.broadcast_to(sq, norm_ref.shape)


def shared_sum(recv, cap):
    return pl.pallas_call(
        functools.partial(shared_kernel, cap),
        in_specs=in_vmem(1),
        out_specs=in_vmem(2),
        out_shape=[
            jax.ShapeDtypeStruct((32, LANES // 2), F32),
            jax.ShapeDtypeStruct((TILE, LANES), F32),
        ],
        compiler_params=params(16),
        name="shared_sum",
    )(recv)


def unpack_kernel(cap, recv_ref, rows_ref, in_t, cot_t):
    n = recv_ref.shape[0]
    count = n * cap
    for k, ref in enumerate((in_t, cot_t)):
        tiles = recv_ref[:, k * cap : (k + 1) * cap].astype(F32)
        ref[...] = tiles.reshape(count * TILE, LANES)
        for j in range(TILE):
            cols = slice(j * LANES, (j + 1) * LANES)
            rows_ref[k, :, cols] = gather_cols(ref, count, j).astype(BF)


def unpack(recv, cap):
    count = recv.shape[0] * cap
    return pl.pallas_call(
        functools.partial(unpack_kernel, cap),
        in_specs=in_vmem(1),
        out_specs=pl.BlockSpec(memory_space=pltpu.VMEM),
        out_shape=jax.ShapeDtypeStruct((2, count, HALF), BF),
        scratch_shapes=[pltpu.VMEM((count * TILE, LANES), F32)] * 2,
        compiler_params=params(16),
        name="unpack",
    )(recv)


def products(side, rows_ref, gate_ref, up_ref, down_ref, sums):
    step = 2 * LANES
    for s in range(0, HALF, step):
        cols = pl.ds(pl.multiple_of(side * HALF + s, step), step)
        a, b = rows_ref[0, :, s : s + step], rows_ref[1, :, s : s + step]
        for k, (x, w) in enumerate(((a, gate_ref), (a, up_ref), (b, down_ref))):
            sums[k] = sums[k] + dot(x, w[0, :, cols], 1, 1)
    return sums


def columns(ref, x, side):
    return ref[0, :, pl.ds(pl.multiple_of((2 * x + side) * LANES, LANES), LANES)]


def half_kernel(core_s, own_ref, gate_ref, up_ref, down_ref, out_ref, give_ref):
    for x in range(give_ref.shape[1] // LANES):
        pair = [columns(ref, x, 1 - core_s[0]) for ref in (gate_ref, up_ref)]
        give_ref[:, x * LANES : (x + 1) * LANES] = jnp.concatenate(pair, axis=0)
    sums = products(core_s[0], own_ref, gate_ref, up_ref, down_ref, [0.0] * 3)
    for k in range(3):
        out_ref[k] = sums[k]


def half_products(core, own, gate, up, down):
    feats = gate.shape[1]
    return pl.pallas_call(
        half_kernel,
        in_specs=in_smem(1) + in_vmem(4),
        out_specs=in_vmem(2),
        out_shape=[
            jax.ShapeDtypeStruct((3, own.shape[1], feats), F32),
            jax.ShapeDtypeStruct((2 * feats, HALF), BF),
        ],
        compiler_params=params(16),
        name="half_products",
    )(core, own, gate, up, down)


def forward_kernel(
    cap, core_s, half_ref, other_ref, gate_ref, up_ref, down_ref, give_ref, hidden_ref
):
    core = core_s[0]
    count = other_ref.shape[1]
    sums = products(1 - core, other_ref, gate_ref, up_ref, down_ref, [half_ref[k] for k in range(3)])
    gate_pre, up_pre, hidden_grad = sums
    sig = jax.nn.sigmoid(gate_pre)
    silu = gate_pre * sig
    hidden = (silu * up_pre).astype(BF)
    hidden_ref[...] = hidden
    up_delta = (hidden_grad * silu).astype(BF)
    gate_delta = (hidden_grad * up_pre * sig * (1.0 + gate_pre * (1.0 - sig))).astype(BF)
    give_ref[:count] = gate_delta
    give_ref[count : 2 * count] = up_delta
    inner = jnp.sum(hidden.astype(F32) * hidden_grad, axis=1, keepdims=True)
    slot = iota((count, LANES), 0)
    lane = (slot // cap) % GROUP * TILE + slot % cap
    spots = jnp.where(lane == iota((count, LANES), 1), inner, 0.0)
    span = GROUP * cap
    lines = [jnp.sum(spots[s : s + span], axis=0, keepdims=True) for s in range(0, count, span)]
    tile = jnp.concatenate(split2(jnp.concatenate(lines, axis=0)), axis=0)
    give_ref[2 * count :] = tile.astype(BF)


def forward(core, half, other, gate, up, down, cap):
    count = other.shape[1]
    feats = gate.shape[1]
    return pl.pallas_call(
        functools.partial(forward_kernel, cap),
        in_specs=in_smem(1) + in_vmem(5),
        out_specs=in_vmem(2),
        out_shape=[
            jax.ShapeDtypeStruct((2 * count + TILE, feats), BF),
            jax.ShapeDtypeStruct((count, feats), BF),
        ],
        compiler_params=params(24),
        name="forward",
    )(core, half, other, gate, up, down)


def shares_kernel(core_s, give_ref, take_ref, cols_ref, gate_ref, up_ref, out_ref):
    count = (give_ref.shape[0] - TILE) // 2
    deltas = [ref[k * count : (k + 1) * count] for ref in (give_ref, take_ref) for k in range(2)]
    deltas = jnp.concatenate(deltas, axis=1)
    last = give_ref[2 * count :].astype(F32) + take_ref[2 * count :].astype(F32)
    inner = split2(last[: TILE // 2] + last[TILE // 2 :])
    inner = jnp.concatenate(inner, axis=0).astype(BF)
    for x in range(out_ref.shape[0]):
        pair = [columns(ref, x, core_s[0]) for ref in (gate_ref, up_ref)]
        pair.append(cols_ref[:, x * LANES : (x + 1) * LANES])
        out_ref[x, :count] = dot(deltas, jnp.concatenate(pair, axis=0)).astype(BF)
        out_ref[x, count:] = inner


def shares(core, give, take, cols, gate, up):
    count = (give.shape[0] - TILE) // 2
    return pl.pallas_call(
        shares_kernel,
        in_specs=in_smem(1) + in_vmem(5),
        out_specs=pl.BlockSpec(memory_space=pltpu.VMEM),
        out_shape=jax.ShapeDtypeStruct((TILE, count + TILE, LANES), BF),
        compiler_params=params(16),
        name="shares",
    )(core, give, take, cols, gate, up)


def grads_kernel(
    core_s, give_ref, hidden_ref, own_ref, other_ref, gate_ref, up_ref, down_ref, norm_ref
):
    core = core_s[0]
    count = hidden_ref.shape[0]
    deltas = (give_ref[:count], give_ref[count : 2 * count], hidden_ref[...])
    step = 2 * LANES
    for k, (out, which) in enumerate(((gate_ref, 0), (up_ref, 0), (down_ref, 1))):
        total = 0.0
        delta = deltas[k].astype(F32).T.astype(BF)
        for side, ref in ((core, own_ref), (1 - core, other_ref)):
            for s in range(0, HALF, step):
                g = dot(delta, ref[which, :, s : s + step])
                cols = pl.ds(pl.multiple_of(side * HALF + s, step), step)
                out[0, :, cols] = g.astype(BF)
                sq = g * g
                total = total + sq[:, :LANES] + sq[:, LANES:]
        norm_ref[k] = jnp.sum(total.T, axis=0, keepdims=True)


def grads(core, give, hidden, own, other):
    feats = hidden.shape[1]
    out = jax.ShapeDtypeStruct((1, feats, 2 * HALF), BF)
    return pl.pallas_call(
        grads_kernel,
        in_specs=in_smem(1) + in_vmem(4),
        out_specs=in_vmem(4),
        out_shape=[out, out, out, jax.ShapeDtypeStruct((3, 1, feats), F32)],
        compiler_params=params(24),
        name="grads",
    )(core, give, hidden, own, other)


def back_kernel(cap, parts_ref, norm_ref, out_ref, sums, rows):
    n = out_ref.shape[0]
    count = n * cap
    total = parts_ref[0].astype(F32)
    for x in range(1, parts_ref.shape[0]):
        total = total + parts_ref[x].astype(F32)
    sums[...] = total
    for r in range(cap):
        rows[pl.ds(r, n, stride=TILE), :] = sums[pl.ds(r, n, stride=cap), :]
    lines = n // GROUP
    inner = split2(total[count : count + lines] + total[count + lines : count + 2 * lines])
    for r, part in zip((cap, cap + 2), inner):
        spread_lines = [
            jnp.broadcast_to(part[g : g + 1], (GROUP, LANES)) for g in range(lines)
        ]
        rows[pl.ds(r, n, stride=TILE), :] = jnp.concatenate(spread_lines, axis=0)
    norm_hi, norm_lo = split2(norm_ref[:1])
    norm = jnp.where(iota((1, LANES), 1) < LANES // 2, norm_hi, norm_lo)
    rows[pl.ds(cap + 1, n, stride=TILE), :] = jnp.broadcast_to(norm, (n, LANES))
    out_ref[...] = rows[...].astype(BF).reshape(n, TILE, LANES)


def back_rows(parts, norms, n, cap):
    return pl.pallas_call(
        functools.partial(back_kernel, cap),
        in_specs=in_vmem(2),
        out_specs=pl.BlockSpec(memory_space=pltpu.VMEM),
        out_shape=jax.ShapeDtypeStruct((n, TILE, LANES), BF),
        scratch_shapes=[
            pltpu.VMEM(parts.shape[1:], F32),
            pltpu.VMEM((n * TILE, LANES), F32),
        ],
        compiler_params=params(16),
        name="back_rows",
    )(parts, norms)


def end_kernel(cap, me_s, recv_ref, ids_ref, slot_ref, w_ref, tok_ref, route_ref, norm_ref):
    n = recv_ref.shape[0]
    count = ids_ref.shape[1]
    rows = recv_ref[...].reshape(n * TILE, LANES)
    o = iota((n * TILE, count), 0)
    ids = [ids_ref[k : k + 1, :] for k in range(2)]
    first = [i * TILE for i in ids]
    rank = [slot_ref[k : k + 1, :] - ids[k] * (2 * cap + SHARED) for k in range(2)]
    pick = ones_at((o == first[0] + rank[0]) | (o == first[1] + rank[1]))
    tok_ref[...] = dot(pick, rows, 0, 0).astype(BF)
    route = []
    for k in range(2):
        pick = ones_at((o == first[k] + cap) | (o == first[k] + cap + 2))
        got = dot(rows, pick, 0, 0)
        use = iota((LANES, count), 0) == (me_s[0] % GROUP) * TILE + rank[k]
        route.append(jnp.sum(jnp.where(use, got, 0.0), axis=0, keepdims=True))
    route_ref[...] = jnp.concatenate(route, axis=0) / w_ref[...]
    sums = dot(ones_at(iota((TILE, n * TILE), 1) % TILE == cap + 1), rows)
    norm_ref[...] = sums[:1, : LANES // 2] + sums[:1, LANES // 2 :]


def end(me, recv, ids_t, slots, w_t, cap):
    count = ids_t.shape[1]
    return pl.pallas_call(
        functools.partial(end_kernel, cap),
        in_specs=in_smem(1) + in_vmem(4),
        out_specs=in_vmem(3),
        out_shape=[
            jax.ShapeDtypeStruct((count, LANES), BF),
            jax.ShapeDtypeStruct((2, count), F32),
            jax.ShapeDtypeStruct((1, LANES // 2), F32),
        ],
        compiler_params=params(16),
        name="end",
    )(me, recv, ids_t, slots, w_t)


def swap(v):
    return lax.ppermute(v, "c", [(0, 1), (1, 0)])


def local(tokens, out_grad, expert_ids, route_weights, gate_proj, up_proj, down_proj, shared_act):
    n = lax.axis_size(EP)
    cap = 5 * tokens.shape[0] * expert_ids.shape[1] // (4 * n)
    core = lax.axis_index("c").reshape(1)
    at = lax.axis_index(TP).reshape(1)
    me = lax.axis_index(EP).reshape(1)
    ids_t, w_t = expert_ids.T, route_weights.T
    here = (tokens, out_grad, shared_act, ids_t, w_t)
    here = [pltpu.with_memory_space_constraint(v, pltpu.HBM) for v in here]
    sent, slots = send_rows(at, me, *here, cap, n)
    recv = lax.all_to_all(sent, EP, 0, 0, tiled=True)
    own = unpack(recv, cap)
    other = swap(own)
    half, cols = half_products(core, own, gate_proj, up_proj, down_proj)
    cols = swap(cols)
    shared, norms = shared_sum(recv, cap)
    give, hidden = forward(core, half, other, gate_proj, up_proj, down_proj, cap)
    part = shares(core, give, swap(give), cols, gate_proj, up_proj)
    part, norms = lax.optimization_barrier((part, norms))
    back = back_rows(lax.all_to_all(part, "x", 0, 0, tiled=True), norms, n, cap)
    back, hidden = lax.optimization_barrier((back, hidden))
    gate_grad, up_grad, down_grad, row_norms = grads(core, give, hidden, own, other)
    returned = lax.all_to_all(back, EP, 0, 0, tiled=True)
    token_grad, route_grad, shared_norms = end(me, returned, ids_t, slots, w_t, cap)
    return (
        token_grad,
        route_grad.T,
        gate_grad,
        up_grad,
        down_grad,
        row_norms.transpose(1, 0, 2),
        shared.T,
        shared_norms.reshape(-1),
    )


def solution(mesh):
    torus = Mesh(mesh.devices.reshape(8, 8, mesh.shape["tp"] // 2, 2), (*EP, *TP))
    return jax.shard_map(
        local,
        mesh=torus,
        in_specs=(
            P(EP, None),
            P(EP, None),
            P(EP, None),
            P(EP, None),
            P(EP, TP, None),
            P(EP, TP, None),
            P(EP, TP, None),
            P(EP, None),
        ),
        out_specs=(
            P(EP, TP),
            P(EP, None),
            P(EP, TP, None),
            P(EP, TP, None),
            P(EP, TP, None),
            P(EP, None, TP),
            P(TP, EP),
            P(TP),
        ),
        check_vma=False,
    )
```
